512 devices in a mesh: sp: 64 (over z, y), tp: 8 (over x, core).
Axes of the slice: x: 4, y: 4, z: 16, core: 2. Of those that a mesh axis runs over, the one named last changes fastest.
Arguments:
- residual: bfloat16 [12288, 2048], P(('sp', 'tp')), may hold values from -6 to 6
- queries: bfloat16 [12288, 1024], P('sp', 'tp'), may hold values from -6 to 6
- key_pairs: bfloat16 [12288, 1024], P('sp', 'tp'), may hold values from -6 to 6
- values: bfloat16 [12288, 1024], P('sp', 'tp'), may hold values from -6 to 6
- second_weight: float32 [8], P('tp'), may hold values from 0.3 to 0.8
- head_gain: float32 [1024], P('tp'), may hold values from 0.1 to 1.9
- out_weight: bfloat16 [1024, 2048], P('tp'), may hold values from -0.1875 to 0.1875
- norm_gain: float32 [2048], replicated, may hold values from 0.1 to 1.9
- up_weight: bfloat16 [2048, 5632], P('sp', 'tp'), may hold values from -0.125 to 0.125
- gate_weight: bfloat16 [2048, 5632], P('sp', 'tp'), may hold values from -0.125 to 0.125
- conv_weight: float32 [3, 5632], P(None, 'tp'), may hold values from -3.5 to 3.5
- conv_bias: float32 [5632], P('tp'), may hold values from -3 to 3
- down_weight: bfloat16 [5632, 2048], P('tp', 'sp'), may hold values from -0.078125 to 0.078125
Outputs:
- layer_out: bfloat16 [12288, 2048], P(('sp', 'tp'))
The draws below stay inside these ranges and needn't reach their ends.
All inputs are finite; a program needn't handle non-finite values.
Results may differ from the reference program's by a relative error of at most 0.017.
Values may be sent and summed in bfloat16 or wider, within the bound.
No kernel may reach another device: no remote copies, remote signals or barrier semaphores. Data moves between devices by JAX's collectives and lax.ppermute only.
A program may use at most 64 MiB of HBM per device.

```python
import math
import jax
import jax.numpy as jnp
from jax import lax

D = 2048
HEADS = 8
HD = 64
VD = 128
FF = 5632
KW = 3
TOKENS = 12288
N_TP = 8


def plant_pairs(key):
    base_key = jax.random.fold_in(key, 101)
    key_q, key_k = jax.random.split(base_key, 2)
    width_all = HEADS * 2 * HD
    query_draw = jax.random.normal(key_q, (TOKENS, width_all), jnp.float32) * 1.3
    key_draw = jax.random.normal(key_k, (TOKENS, width_all), jnp.float32) * 1.3
    return (jnp.clip(query_draw, -6.0, 6.0), jnp.clip(key_draw, -6.0, 6.0))


def draw_queries(key, part):
    return plant_pairs(key)[0].astype(jnp.bfloat16)


def draw_key_pairs(key, part):
    return plant_pairs(key)[1].astype(jnp.bfloat16)


def steps_of(stream_key, extent, cuts, least, high):
    loudness = 1.0
    for position, blocks in cuts:
        draws = jax.random.uniform(jax.random.fold_in(jax.random.fold_in(stream_key, 6), position), (blocks,), jnp.float32, least / len(cuts), high / len(cuts))
        loudness = loudness * jnp.repeat(jnp.exp(draws), extent[position] // blocks).reshape((-1,) + (1,) * (len(extent) - 1 - position))
    return loudness


def normal_values(key, extent, spread, bound, cuts=(), held_as=jnp.bfloat16):
    entries = jax.random.normal(key, extent, jnp.float32) * spread
    if len(cuts) > 0:
        entries = steps_of(key, extent, cuts, -0.22, 0.18) * entries
    return jnp.clip(entries, min=-bound, max=bound).astype(held_as)


def setup_inputs(seed: int = 0) -> dict:
    key_list = jax.random.split(jax.random.key(seed), 14)
    return {
        "residual": normal_values(key_list[0], (TOKENS, D), 1.0, 6.0, ((0, 512),)),
        "queries": draw_queries(jax.random.fold_in(key_list[13], 71), 0),
        "key_pairs": draw_key_pairs(jax.random.fold_in(key_list[13], 71), 0),
        "values": normal_values(key_list[3], (TOKENS, HEADS * VD), 1.0, 6.0, ((0, 64), (1, 8))),
        "second_weight": jnp.clip(0.3 + 0.5 * jax.random.uniform(key_list[4], (HEADS,), jnp.float32) ** steps_of(key_list[4], (HEADS,), ((0, 8),), -0.2, 0.2), 0.3, 0.8),
        "head_gain": jnp.clip(1.0 + 0.18 * jax.random.normal(key_list[5], (HEADS * VD,), jnp.float32), 0.1, 1.9),
        "out_weight": normal_values(key_list[6], (HEADS * VD, D), (HEADS * VD) ** -0.5, 0.1875, ((0, 8),)),
        "norm_gain": jnp.clip(1.0 + 0.18 * jax.random.normal(key_list[7], (D,), jnp.float32), 0.1, 1.9),
        "up_weight": normal_values(key_list[8], (D, FF), D ** -0.5, 0.125, ((0, 64), (1, 8))),
        "gate_weight": normal_values(key_list[9], (D, FF), D ** -0.5, 0.125, ((0, 64), (1, 8))),
        "conv_weight": normal_values(key_list[10], (KW, FF), KW ** -0.5, 3.5, ((1, 8),), jnp.float32),
        "conv_bias": normal_values(key_list[11], (FF,), 0.5, 3.0, ((0, 8),), jnp.float32),
        "down_weight": normal_values(key_list[12], (FF, D), FF ** -0.5, 0.078125, ((0, 8), (1, 64))),
    }


eps = 1e-05
neg_fill = -1e+30

def normalize(rows_in, gain):
    values_f = rows_in.astype(jnp.float32)
    scale_inv = lax.rsqrt(lax.optimization_barrier(jnp.mean(values_f * values_f, axis=-1, keepdims=True)) + eps)
    return (values_f * scale_inv * gain).astype(jnp.bfloat16)

def reference(residual, queries, key_pairs, values, second_weight, head_gain, out_weight, norm_gain, up_weight, gate_weight, conv_weight, conv_bias, down_weight):
    block_size = math.gcd(TOKENS, 512)
    block_count = TOKENS // block_size
    query_all = queries.astype(jnp.float32).reshape(TOKENS, HEADS, 2, HD)
    key_all = key_pairs.astype(jnp.float32).reshape(TOKENS, HEADS, 2, HD)
    value_all = values.astype(jnp.float32).reshape(TOKENS, HEADS, VD)
    key_pos = jnp.arange(TOKENS).astype(jnp.int32)
    gain_heads = head_gain.reshape(HEADS, VD)

    def attend_block(index_block):
        first = (index_block * block_size).astype(jnp.int32)
        query_block = lax.dynamic_slice_in_dim(query_all, first, block_size, 0)
        positions = first + jnp.arange(block_size).astype(jnp.int32)
        scores = jnp.einsum('qhmd,khmd->hmqk', query_block, key_all) * HD ** (-0.5)
        visible = key_pos[None, :] <= positions[:, None]
        scores = jnp.where(visible, scores, neg_fill)
        maxima = lax.optimization_barrier(jnp.max(scores, axis=-1, keepdims=True))
        exp_scores = jnp.where(visible, jnp.exp(scores - maxima), jnp.float32(0.0))
        totals = lax.optimization_barrier(jnp.sum(exp_scores, axis=-1))
        rounded = exp_scores.astype(jnp.bfloat16).astype(jnp.float32)
        weighted = jnp.einsum('hmqk,khe->hmqe', rounded, value_all)
        diff = weighted[:, 0] / totals[:, 0, :, None] - second_weight[:, None, None] * weighted[:, 1] / totals[:, 1, :, None]
        diff = jnp.transpose(diff, (1, 0, 2))
        scale_inv = lax.rsqrt(lax.optimization_barrier(jnp.mean(diff * diff, axis=-1, keepdims=True)) + eps)
        normed_heads = diff * scale_inv * gain_heads * 0.8
        return normed_heads.reshape(block_size, HEADS * VD).astype(jnp.bfloat16)
    attended = lax.map(attend_block, jnp.arange(block_count).astype(jnp.int32)).reshape(TOKENS, HEADS * VD)
    group_rows = HEADS * VD // N_TP
    proj_sum = jnp.zeros((TOKENS, D), jnp.float32)
    for group in range(N_TP):
        part_prod = jnp.dot(attended[:, group * group_rows:(group + 1) * group_rows], out_weight[group * group_rows:(group + 1) * group_rows], preferred_element_type=jnp.float32)
        proj_sum = proj_sum + part_prod.astype(jnp.bfloat16).astype(jnp.float32)
    proj = proj_sum.astype(jnp.bfloat16)
    mid = (residual.astype(jnp.float32) + proj.astype(jnp.float32)).astype(jnp.bfloat16)
    normed = normalize(mid, norm_gain)
    up_proj = jnp.dot(normed, up_weight, preferred_element_type=jnp.float32).astype(jnp.bfloat16)
    gate_proj = jnp.dot(normed, gate_weight, preferred_element_type=jnp.float32).astype(jnp.bfloat16)
    padded = jnp.pad(up_proj.astype(jnp.float32), ((KW - 1, 0), (0, 0)))
    conv_out = jnp.zeros((TOKENS, FF), jnp.float32) + conv_bias
    for tap in range(KW):
        conv_out = conv_out + conv_weight[tap] * padded[tap:tap + TOKENS]
    hidden = (jax.nn.silu(conv_out) * gate_proj.astype(jnp.float32)).astype(jnp.bfloat16)
    group_units = FF // N_TP
    ffn_sum = jnp.zeros((TOKENS, D), jnp.float32)
    for group in range(N_TP):
        part_prod = jnp.dot(hidden[:, group * group_units:(group + 1) * group_units], down_weight[group * group_units:(group + 1) * group_units], preferred_element_type=jnp.float32)
        ffn_sum = ffn_sum + part_prod.astype(jnp.bfloat16).astype(jnp.float32)
    ffn_out = ffn_sum.astype(jnp.bfloat16)
    return (mid.astype(jnp.float32) + ffn_out.astype(jnp.float32)).astype(jnp.bfloat16)
```

```python
import jax
import jax.numpy as jnp
from jax import lax
from jax.experimental import pallas as pl
from jax.experimental.pallas import tpu as pltpu
from jax.sharding import Mesh
from jax.sharding import PartitionSpec as P

HD = 64
VD = 128
SP = ("z", "y")
SP_TP = ("z", "y", "tp")
NZ = 16
NY = 4
eps = 1e-05
neg_fill = -1e30
TILE = 128
FAR = (4, 8, 12)
NEAR = ((1, 5, 9, 13), (2, 6, 10, 14), (3, 7, 11, 15))

VMEM = pl.BlockSpec(memory_space=pltpu.VMEM)
SMEM = pl.BlockSpec(memory_space=pltpu.SMEM)


def shifted(value, axis, steps):
    count = lax.axis_size(axis)
    return lax.ppermute(value, axis, [(i, (i + steps) % count) for i in range(count)])


def dot_nt(a, b):
    return lax.dot_general(a, b, (((1,), (1,)), ((), ())), preferred_element_type=jnp.float32)


def attend_kernel(where_ref, q_ref, own_ref, far_ref, n1_ref, n2_ref, n3_ref, out_ref):
    z = where_ref[0]
    y = where_ref[1]
    rows = own_ref.shape[0]

    def row_bias(offsets):
        lane = lax.broadcasted_iota(jnp.int32, (1, rows * len(offsets)), 1)
        bias = jnp.zeros(lane.shape, jnp.float32)
        for i, off in enumerate(offsets):
            inside = jnp.logical_and(lane >= i * rows, lane < (i + 1) * rows)
            bias = jnp.where(jnp.logical_and(inside, off > z), neg_fill, bias)
        return bias

    pieces = ((far_ref, FAR), (n1_ref, NEAR[0]), (n2_ref, NEAR[1]), (n3_ref, NEAR[2]))
    biases = [row_bias(offsets) for _, offsets in pieces]
    lane_q = lax.broadcasted_iota(jnp.int32, (TILE, 2 * HD), 1)
    lane_s = lax.broadcasted_iota(jnp.int32, (TILE, VD), 1)

    @pl.loop(0, NY * rows // TILE)
    def _(t):
        at = pl.multiple_of(t * TILE, TILE)
        q = q_ref[pl.ds(at, TILE), :] * jnp.bfloat16(HD**-0.5)
        zero = jnp.zeros_like(q)
        q2 = jnp.concatenate(
            (jnp.where(lane_q < HD, q, zero), jnp.where(lane_q < HD, zero, q)), axis=0
        )
        s_own = dot_nt(q2, own_ref[:, : 2 * HD])
        r = lax.broadcasted_iota(jnp.int32, s_own.shape, 0)
        r = jnp.where(r >= TILE, r - TILE, r) + at
        k = lax.broadcasted_iota(jnp.int32, s_own.shape, 1) + y * rows
        s_own = jnp.where(k <= r, s_own, neg_fill)
        scores = [s_own] + [
            dot_nt(q2, ref[:, : 2 * HD]) + bias for (ref, _), bias in zip(pieces, biases)
        ]
        top = jnp.max(scores[0], axis=1, keepdims=True)
        for s in scores[1:]:
            top = jnp.maximum(top, jnp.max(s, axis=1, keepdims=True))
        total = jnp.zeros((2 * TILE, 1), jnp.float32)
        acc = jnp.zeros((2 * TILE, VD), jnp.float32)
        for s, ref in zip(scores, (own_ref, far_ref, n1_ref, n2_ref, n3_ref)):
            e = jnp.exp(s - top)
            total = total + jnp.sum(e, axis=1, keepdims=True)
            acc = acc + jnp.dot(
                e.astype(jnp.bfloat16), ref[:, 2 * HD :], preferred_element_type=jnp.float32
            )
        mean = acc / total
        lse = top + jnp.log(total)
        hi = lse.astype(jnp.bfloat16).astype(jnp.float32)
        mid = (lse - hi).astype(jnp.bfloat16).astype(jnp.float32)
        low = lse - hi - mid
        stat = jnp.zeros((TILE, VD), jnp.float32)
        for m in range(2):
            for i, v in enumerate((hi, mid, low)):
                stat = jnp.where(lane_s == 3 * m + i, v[m * TILE : (m + 1) * TILE], stat)
        out_ref[pl.ds(at, TILE), 0:VD] = mean[:TILE].astype(jnp.bfloat16)
        out_ref[pl.ds(at, TILE), VD : 2 * VD] = mean[TILE:].astype(jnp.bfloat16)
        out_ref[pl.ds(at, TILE), 2 * VD : 3 * VD] = stat.astype(jnp.bfloat16)


def project_kernel(weight2_ref, got_ref, gain_ref, out_w_ref, out_ref):
    means = []
    for m in range(2):
        lses = []
        for y in range(NY):
            part = got_ref[y, :, 2 * VD + 3 * m : 2 * VD + 3 * m + 3].astype(jnp.float32)
            lses.append(part[:, 0:1] + part[:, 1:2] + part[:, 2:3])
        top = lses[0]
        for v in lses[1:]:
            top = jnp.maximum(top, v)
        total = jnp.zeros_like(top)
        acc = jnp.zeros((top.shape[0], VD), jnp.float32)
        for y in range(NY):
            share = jnp.exp(lses[y] - top)
            total = total + share
            acc = acc + share * got_ref[y, :, m * VD : (m + 1) * VD].astype(jnp.float32)
        means.append(acc / total)
    diff = means[0] - weight2_ref[0] * means[1]
    scale_inv = lax.rsqrt(jnp.mean(diff * diff, axis=-1, keepdims=True) + eps)
    attended = (diff * scale_inv * gain_ref[...] * 0.8).astype(jnp.bfloat16)
    out_ref[...] = jnp.dot(attended, out_w_ref[...], preferred_element_type=jnp.float32).astype(
        jnp.bfloat16
    )


def mid_kernel(parts_ref, residual_ref, gain_ref, mid_ref, normed_ref):
    proj = parts_ref[0].astype(jnp.float32)
    for i in range(1, parts_ref.shape[0]):
        proj = proj + parts_ref[i].astype(jnp.float32)
    proj = proj.astype(jnp.bfloat16).astype(jnp.float32)
    mid = (residual_ref[...].astype(jnp.float32) + proj).astype(jnp.bfloat16)
    mid_ref[...] = mid
    mid_f = mid.astype(jnp.float32)
    scale_inv = lax.rsqrt(jnp.mean(mid_f * mid_f, axis=-1, keepdims=True) + eps)
    normed_ref[...] = (mid_f * scale_inv * gain_ref[...]).astype(jnp.bfloat16)


def last_kernel(parts_ref, mid_ref, out_ref):
    ffn = parts_ref[0].astype(jnp.float32)
    for i in range(1, parts_ref.shape[0]):
        ffn = ffn + parts_ref[i].astype(jnp.float32)
    ffn = ffn.astype(jnp.bfloat16).astype(jnp.float32)
    out_ref[...] = (mid_ref[...].astype(jnp.float32) + ffn).astype(jnp.bfloat16)


def local(
    residual,
    queries,
    key_pairs,
    values,
    second_weight,
    head_gain,
    out_weight,
    norm_gain,
    up_weight,
    gate_weight,
    conv_weight,
    conv_bias,
    down_weight,
):
    rows = queries.shape[0]
    ff = up_weight.shape[1]
    d = residual.shape[1]
    tp = lax.axis_size("tp")
    where = jnp.stack((lax.axis_index("z"), lax.axis_index("y"))).astype(jnp.int32)
    own_w = jnp.concatenate((up_weight, gate_weight, down_weight.T), axis=1)
    row_w = lax.all_gather(own_w, "y", axis=0, tiled=True)
    all_w = lax.all_gather(row_w, "z", axis=0, tiled=True)

    kv = jnp.concatenate((key_pairs, values), axis=1)
    q_all = lax.all_gather(queries, "y", axis=0, tiled=True)
    f4, f8, f12 = (shifted(kv, "z", s) for s in (4, 8, -4))
    held = jnp.concatenate((kv, f4, f8, f12), axis=0)
    n1 = shifted(held, "z", 1)
    n2a = shifted(held[: 2 * rows], "z", 2)
    back = jnp.concatenate((f12, kv), axis=0)
    n2b = shifted(back, "z", -2)
    n2 = jnp.concatenate((n2a, n2b), axis=0)
    n3 = shifted(jnp.concatenate((f4, f8, f12, kv), axis=0), "z", -1)
    far = held[rows:]
    parts = pl.pallas_call(
        attend_kernel,
        out_shape=jax.ShapeDtypeStruct((NY * rows, 3 * VD), jnp.bfloat16),
        in_specs=[SMEM] + [VMEM] * 6,
        out_specs=VMEM,
        name="attend",
    )(where, q_all, kv, far, n1, n2, n3)
    got = lax.all_to_all(parts.reshape(NY, rows, 3 * VD), "y", 0, 0, tiled=True)
    proj = pl.pallas_call(
        project_kernel,
        out_shape=jax.ShapeDtypeStruct((rows, d), jnp.bfloat16),
        in_specs=[SMEM] + [VMEM] * 3,
        out_specs=VMEM,
        name="project",
    )(second_weight, got, head_gain.reshape(1, VD), out_weight)
    proj_parts = lax.all_to_all(proj.reshape(tp, rows // tp, d), "tp", 0, 0, tiled=True)
    mid, normed = pl.pallas_call(
        mid_kernel,
        out_shape=[jax.ShapeDtypeStruct((rows // tp, d), jnp.bfloat16)] * 2,
        in_specs=[VMEM] * 3,
        out_specs=[VMEM] * 2,
        name="mid",
    )(proj_parts, residual, norm_gain.reshape(1, d))
    normed_all = lax.all_gather(normed, "tp", axis=0, tiled=True)
    both = jnp.dot(normed_all, all_w[:, : 2 * ff], preferred_element_type=jnp.float32).astype(
        jnp.bfloat16
    )
    up_proj, gate_proj = both[:, :ff], both[:, ff:]
    taps = conv_weight.shape[0]
    count = lax.axis_size("z") * lax.axis_size("y")
    rim_rows = lax.ppermute(
        up_proj[rows - (taps - 1) :], SP, [(i, i + 1) for i in range(count - 1)]
    )
    extended = jnp.concatenate((rim_rows, up_proj), axis=0)
    conv_out = jnp.zeros((rows, ff), jnp.float32) + conv_bias[None, :]
    for tap in range(taps):
        conv_out = conv_out + conv_weight[tap][None, :] * extended[tap : tap + rows].astype(
            jnp.float32
        )
    hidden = (jax.nn.silu(conv_out) * gate_proj.astype(jnp.float32)).astype(jnp.bfloat16)
    ffn = dot_nt(hidden, all_w[:, 2 * ff :]).astype(jnp.bfloat16)
    ffn_parts = lax.all_to_all(ffn.reshape(tp, rows // tp, d), "tp", 0, 0, tiled=True)
    return pl.pallas_call(
        last_kernel,
        out_shape=jax.ShapeDtypeStruct((rows // tp, d), jnp.bfloat16),
        in_specs=[VMEM] * 2,
        out_specs=VMEM,
        name="last",
    )(ffn_parts, mid)


def solution(mesh):
    finer = Mesh(mesh.devices.reshape(NZ, NY, mesh.shape["tp"]), ("z", "y", "tp"))
    in_specs = (
        P(SP_TP, None),
        P(SP, "tp"),
        P(SP, "tp"),
        P(SP, "tp"),
        P("tp"),
        P("tp"),
        P("tp", None),
        P(),
        P(SP, "tp"),
        P(SP, "tp"),
        P(None, "tp"),
        P("tp"),
        P("tp", SP),
    )
    out_specs = P(SP_TP, None)
    return jax.shard_map(local, mesh=finer, in_specs=in_specs, out_specs=out_specs, check_vma=False)
```

```python
import jax
import jax.numpy as jnp
from jax import lax
from jax.experimental import pallas as pl
from jax.experimental.pallas import tpu as pltpu
from jax.sharding import Mesh
from jax.sharding import PartitionSpec as P

HD = 64
VD = 128
SP = ("z", "y")
SP_TP = ("z", "y", "tp")
NZ = 16
NY = 4
eps = 1e-05
neg_fill = -1e30
TILE = 128
FAR = (4, 8, 12)
NEAR = ((1, 5, 9, 13), (2, 6, 10, 14), (3, 7, 11, 15))

VMEM = pl.BlockSpec(memory_space=pltpu.VMEM)
SMEM = pl.BlockSpec(memory_space=pltpu.SMEM)


def shifted(value, axis, steps):
    count = lax.axis_size(axis)
    return lax.ppermute(value, axis, [(i, (i + steps) % count) for i in range(count)])


def dot_nt(a, b):
    return lax.dot_general(a, b, (((1,), (1,)), ((), ())), preferred_element_type=jnp.float32)


def attend_kernel(where_ref, q_ref, own_ref, far_ref, n1_ref, n2_ref, n3_ref, out_ref):
    z = where_ref[0]
    y = where_ref[1]
    rows = own_ref.shape[0]

    def row_bias(offsets):
        lane = lax.broadcasted_iota(jnp.int32, (1, rows * len(offsets)), 1)
        bias = jnp.zeros(lane.shape, jnp.float32)
        for i, off in enumerate(offsets):
            inside = jnp.logical_and(lane >= i * rows, lane < (i + 1) * rows)
            bias = jnp.where(jnp.logical_and(inside, off > z), neg_fill, bias)
        return bias

    pieces = ((far_ref, FAR), (n1_ref, NEAR[0]), (n2_ref, NEAR[1]), (n3_ref, NEAR[2]))
    biases = [row_bias(offsets) for _, offsets in pieces]
    lane_q = lax.broadcasted_iota(jnp.int32, (TILE, 2 * HD), 1)
    lane_s = lax.broadcasted_iota(jnp.int32, (TILE, VD), 1)

    @pl.loop(0, NY * rows // TILE)
    def _(t):
        at = pl.multiple_of(t * TILE, TILE)
        q = q_ref[pl.ds(at, TILE), :] * jnp.bfloat16(HD**-0.5)
        zero = jnp.zeros_like(q)
        q2 = jnp.concatenate(
            (jnp.where(lane_q < HD, q, zero), jnp.where(lane_q < HD, zero, q)), axis=0
        )
        s_own = dot_nt(q2, own_ref[:, : 2 * HD])
        r = lax.broadcasted_iota(jnp.int32, s_own.shape, 0)
        r = jnp.where(r >= TILE, r - TILE, r) + at
        k = lax.broadcasted_iota(jnp.int32, s_own.shape, 1) + y * rows
        s_own = jnp.where(k <= r, s_own, neg_fill)
        scores = [s_own] + [
            dot_nt(q2, ref[:, : 2 * HD]) + bias for (ref, _), bias in zip(pieces, biases)
        ]
        top = jnp.max(scores[0], axis=1, keepdims=True)
        for s in scores[1:]:
            top = jnp.maximum(top, jnp.max(s, axis=1, keepdims=True))
        total = jnp.zeros((2 * TILE, 1), jnp.float32)
        acc = jnp.zeros((2 * TILE, VD), jnp.float32)
        for s, ref in zip(scores, (own_ref, far_ref, n1_ref, n2_ref, n3_ref)):
            e = jnp.exp(s - top)
            total = total + jnp.sum(e, axis=1, keepdims=True)
            acc = acc + jnp.dot(
                e.astype(jnp.bfloat16), ref[:, 2 * HD :], preferred_element_type=jnp.float32
            )
        mean = acc / total
        lse = top + jnp.log(total)
        hi = lse.astype(jnp.bfloat16).astype(jnp.float32)
        mid = (lse - hi).astype(jnp.bfloat16).astype(jnp.float32)
        low = lse - hi - mid
        stat = jnp.zeros((TILE, VD), jnp.float32)
        for m in range(2):
            for i, v in enumerate((hi, mid, low)):
                stat = jnp.where(lane_s == 3 * m + i, v[m * TILE : (m + 1) * TILE], stat)
        out_ref[pl.ds(at, TILE), 0:VD] = mean[:TILE].astype(jnp.bfloat16)
        out_ref[pl.ds(at, TILE), VD : 2 * VD] = mean[TILE:].astype(jnp.bfloat16)
        out_ref[pl.ds(at, TILE), 2 * VD : 3 * VD] = stat.astype(jnp.bfloat16)


def merged(got):
    got = got.astype(jnp.float32)
    means = []
    for m in range(2):
        stat = got[:, :, 2 * VD + 3 * m : 2 * VD + 3 * m + 3]
        lse = stat[..., 0:1] + stat[..., 1:2] + stat[..., 2:3]
        share = jnp.exp(lse - jnp.max(lse, axis=0, keepdims=True))
        acc = jnp.sum(share * got[:, :, m * VD : (m + 1) * VD], axis=0)
        means.append(acc / jnp.sum(share, axis=0))
    return means


def normalize(rows_in, gain):
    values_f = rows_in.astype(jnp.float32)
    scale_inv = lax.rsqrt(jnp.mean(values_f * values_f, axis=-1, keepdims=True) + eps)
    return (values_f * scale_inv * gain).astype(jnp.bfloat16)


def summed_over_tp(shard):
    count = lax.axis_size("tp")
    cut = shard.reshape(count, shard.shape[0] // count, shard.shape[1])
    tiles = lax.all_to_all(cut, "tp", 0, 0, tiled=True)
    return jnp.sum(tiles.astype(jnp.float32), axis=0).astype(jnp.bfloat16)


def local(
    residual,
    queries,
    key_pairs,
    values,
    second_weight,
    head_gain,
    out_weight,
    norm_gain,
    up_weight,
    gate_weight,
    conv_weight,
    conv_bias,
    down_weight,
):
    rows = queries.shape[0]
    ff = up_weight.shape[1]
    where = jnp.stack((lax.axis_index("z"), lax.axis_index("y"))).astype(jnp.int32)
    own_w = jnp.concatenate((up_weight, gate_weight, down_weight.T), axis=1)
    row_w = lax.all_gather(own_w, "y", axis=0, tiled=True)
    all_w = lax.all_gather(row_w, "z", axis=0, tiled=True)

    kv = jnp.concatenate((key_pairs, values), axis=1)
    q_all = lax.all_gather(queries, "y", axis=0, tiled=True)
    f4, f8, f12 = (shifted(kv, "z", s) for s in (4, 8, -4))
    f4, f8, f12, q_all = lax.optimization_barrier((f4, f8, f12, q_all))
    held = jnp.concatenate((kv, f4, f8, f12), axis=0)
    n1 = shifted(held, "z", 1)
    n2a = shifted(held[: 2 * rows], "z", 2)
    back = jnp.concatenate((f12, kv), axis=0)
    n2b = shifted(back, "z", -2)
    n2 = jnp.concatenate((n2a, n2b), axis=0)
    n3 = shifted(jnp.concatenate((f4, f8, f12, kv), axis=0), "z", -1)
    far = held[rows:]
    parts = pl.pallas_call(
        attend_kernel,
        out_shape=jax.ShapeDtypeStruct((NY * rows, 3 * VD), jnp.bfloat16),
        in_specs=[SMEM] + [VMEM] * 6,
        out_specs=VMEM,
        name="attend",
    )(where, q_all, kv, far, n1, n2, n3)
    got = lax.all_to_all(parts.reshape(NY, rows, 3 * VD), "y", 0, 0, tiled=True)
    means = merged(got)
    diff = means[0] - second_weight[0] * means[1]
    scale_inv = lax.rsqrt(jnp.mean(diff * diff, axis=-1, keepdims=True) + eps)
    attended = (diff * scale_inv * head_gain * 0.8).astype(jnp.bfloat16)
    proj = summed_over_tp(
        jnp.dot(attended, out_weight, preferred_element_type=jnp.float32).astype(jnp.bfloat16)
    )
    mid = (residual.astype(jnp.float32) + proj.astype(jnp.float32)).astype(jnp.bfloat16)
    normed_all = lax.all_gather(normalize(mid, norm_gain), "tp", axis=0, tiled=True)
    count = lax.axis_size("z") * lax.axis_size("y")
    rim_rows = lax.ppermute(normed_all[rows - 8 :], SP, [(i, i + 1) for i in range(count - 1)])
    both = jnp.dot(
        jnp.concatenate((normed_all, rim_rows), axis=0),
        all_w[:, : 2 * ff],
        preferred_element_type=jnp.float32,
    ).astype(jnp.bfloat16)
    up_proj, gate_proj = both[:rows, :ff], both[:rows, ff:]
    taps = conv_weight.shape[0]
    extended = jnp.concatenate((both[rows + 8 - (taps - 1) :, :ff], up_proj), axis=0)
    conv_out = jnp.zeros((rows, ff), jnp.float32) + conv_bias[None, :]
    for tap in range(taps):
        conv_out = conv_out + conv_weight[tap][None, :] * extended[tap : tap + rows].astype(
            jnp.float32
        )
    hidden = (jax.nn.silu(conv_out) * gate_proj.astype(jnp.float32)).astype(jnp.bfloat16)
    ffn = dot_nt(hidden, all_w[:, 2 * ff :]).astype(jnp.bfloat16)
    ffn_out = summed_over_tp(ffn)
    return (mid.astype(jnp.float32) + ffn_out.astype(jnp.float32)).astype(jnp.bfloat16)


def solution(mesh):
    finer = Mesh(mesh.devices.reshape(NZ, NY, mesh.shape["tp"]), ("z", "y", "tp"))
    in_specs = (
        P(SP_TP, None),
        P(SP, "tp"),
        P(SP, "tp"),
        P(SP, "tp"),
        P("tp"),
        P("tp"),
        P("tp", None),
        P(),
        P(SP, "tp"),
        P(SP, "tp"),
        P(None, "tp"),
        P("tp"),
        P("tp", SP),
    )
    out_specs = P(SP_TP, None)
    return jax.shard_map(local, mesh=finer, in_specs=in_specs, out_specs=out_specs, check_vma=False)
```

```python
import jax
import jax.numpy as jnp
from jax import lax
from jax.experimental import pallas as pl
from jax.experimental.pallas import tpu as pltpu
from jax.sharding import Mesh
from jax.sharding import PartitionSpec as P

HD = 64
VD = 128
SP = ("z", "yh", "yl")
TP = ("x", "c")
Y = ("yh", "yl")
SHARDS = ("x", "yl")
NY = 4
LANES = 128
eps = 1e-05
neg_fill = -1e30
TILE = 128
FAR = (4, 8, 12)
NEAR = ((1, 5, 9, 13), (2, 6, 10, 14), (3, 7, 11, 15))

VMEM = pl.BlockSpec(memory_space=pltpu.VMEM)
SMEM = pl.BlockSpec(memory_space=pltpu.SMEM)


def shifted(value, axis, steps):
    count = lax.axis_size(axis)
    return lax.ppermute(value, axis, [(i, (i + steps) % count) for i in range(count)])


def swapped(value):
    return lax.ppermute(value, ("yl", "c"), [(0, 0), (1, 2), (2, 1), (3, 3)])


def dot_nt(a, b):
    return lax.dot_general(a, b, (((1,), (1,)), ((), ())), preferred_element_type=jnp.float32)


def attend_kernel(where_ref, q_ref, own_ref, far_ref, n1_ref, n2_ref, n3_ref, out_ref):
    z = where_ref[0]
    y = where_ref[1]
    rows = own_ref.shape[0]

    def row_bias(offsets):
        lane = lax.broadcasted_iota(jnp.int32, (1, rows * len(offsets)), 1)
        bias = jnp.zeros(lane.shape, jnp.float32)
        for i, off in enumerate(offsets):
            inside = jnp.logical_and(lane >= i * rows, lane < (i + 1) * rows)
            bias = jnp.where(jnp.logical_and(inside, off > z), neg_fill, bias)
        return bias

    pieces = ((far_ref, FAR), (n1_ref, NEAR[0]), (n2_ref, NEAR[1]), (n3_ref, NEAR[2]))
    biases = [row_bias(offsets) for _, offsets in pieces]
    lane_q = lax.broadcasted_iota(jnp.int32, (TILE, 2 * HD), 1)
    lane_s = lax.broadcasted_iota(jnp.int32, (TILE, VD), 1)

    @pl.loop(0, NY * rows // TILE)
    def _(t):
        at = pl.multiple_of(t * TILE, TILE)
        q = q_ref[pl.ds(at, TILE), :] * jnp.bfloat16(HD**-0.5)
        zero = jnp.zeros_like(q)
        q2 = jnp.concatenate(
            (jnp.where(lane_q < HD, q, zero), jnp.where(lane_q < HD, zero, q)), axis=0
        )
        s_own = dot_nt(q2, own_ref[:, : 2 * HD])
        r = lax.broadcasted_iota(jnp.int32, s_own.shape, 0)
        r = jnp.where(r >= TILE, r - TILE, r) + at
        k = lax.broadcasted_iota(jnp.int32, s_own.shape, 1) + y * rows
        s_own = jnp.where(k <= r, s_own, neg_fill)
        scores = [s_own] + [
            dot_nt(q2, ref[:, : 2 * HD]) + bias for (ref, _), bias in zip(pieces, biases)
        ]
        top = jnp.max(scores[0], axis=1, keepdims=True)
        for s in scores[1:]:
            top = jnp.maximum(top, jnp.max(s, axis=1, keepdims=True))
        total = jnp.zeros((2 * TILE, 1), jnp.float32)
        acc = jnp.zeros((2 * TILE, VD), jnp.float32)
        for s, ref in zip(scores, (own_ref, far_ref, n1_ref, n2_ref, n3_ref)):
            e = jnp.exp(s - top)
            total = total + jnp.sum(e, axis=1, keepdims=True)
            acc = acc + jnp.dot(
                e.astype(jnp.bfloat16), ref[:, 2 * HD :], preferred_element_type=jnp.float32
            )
        mean = acc / total
        lse = top + jnp.log(total)
        hi = lse.astype(jnp.bfloat16).astype(jnp.float32)
        mid = (lse - hi).astype(jnp.bfloat16).astype(jnp.float32)
        low = lse - hi - mid
        stat = jnp.zeros((TILE, VD), jnp.float32)
        for m in range(2):
            for i, v in enumerate((hi, mid, low)):
                stat = jnp.where(lane_s == 3 * m + i, v[m * TILE : (m + 1) * TILE], stat)
        out_ref[pl.ds(at, TILE), 0:VD] = mean[:TILE].astype(jnp.bfloat16)
        out_ref[pl.ds(at, TILE), VD : 2 * VD] = mean[TILE:].astype(jnp.bfloat16)
        out_ref[pl.ds(at, TILE), 2 * VD : 3 * VD] = stat.astype(jnp.bfloat16)


def merged(got):
    got = got.astype(jnp.float32)
    means = []
    for m in range(2):
        stat = got[:, :, 2 * VD + 3 * m : 2 * VD + 3 * m + 3]
        lse = stat[..., 0:1] + stat[..., 1:2] + stat[..., 2:3]
        share = jnp.exp(lse - jnp.max(lse, axis=0, keepdims=True))
        acc = jnp.sum(share * got[:, :, m * VD : (m + 1) * VD], axis=0)
        means.append(acc / jnp.sum(share, axis=0))
    return means


def normalize(rows_in, gain):
    values_f = rows_in.astype(jnp.float32)
    scale_inv = lax.rsqrt(jnp.mean(values_f * values_f, axis=-1, keepdims=True) + eps)
    return (values_f * scale_inv * gain).astype(jnp.bfloat16)


def summed_over_shards(shard):
    count = lax.axis_size(SHARDS)
    cut = shard.reshape(count, shard.shape[0] // count, shard.shape[1])
    tiles = lax.all_to_all(cut, SHARDS, 0, 0, tiled=True)
    return jnp.sum(tiles.astype(jnp.float32), axis=0).astype(jnp.bfloat16)


def local(
    residual,
    queries,
    key_pairs,
    values,
    second_weight,
    head_gain,
    out_weight,
    norm_gain,
    up_weight,
    gate_weight,
    conv_weight,
    conv_bias,
    down_weight,
):
    rows = queries.shape[0]
    ff = up_weight.shape[1]
    half = ff // 2
    core = lax.axis_index("c")
    pair = lax.axis_index("yl")
    y_index = lax.axis_index("yh") * 2 + pair
    where = jnp.stack((lax.axis_index("z"), y_index)).astype(jnp.int32)

    down_t = down_weight.T
    gap = -2 * half % LANES
    width = 2 * half + gap + half
    tail = -width % LANES
    cuts = []
    for h in range(2):
        units = slice(h * half, (h + 1) * half)
        cuts += [up_weight[:, units], gate_weight[:, units]]
        cuts += [jnp.zeros((up_weight.shape[0], gap), jnp.bfloat16), down_t[:, units]]
        cuts += [jnp.zeros((up_weight.shape[0], tail), jnp.bfloat16)]
    row_w = lax.all_gather(jnp.concatenate(cuts, axis=1), Y, axis=0, tiled=True)
    low, high = row_w[:, : width + tail], row_w[:, width + tail :]
    for_peer = lax.ppermute(jnp.where(core == 0, high, low), ("yl", "c"), [(0, 1), (3, 2)])
    kept = jnp.where(core == pair, jnp.where(core == 0, low, high), for_peer)
    mine = lax.all_gather(kept, "z", axis=0, tiled=True)

    kv = jnp.concatenate((key_pairs, values), axis=1)
    q_all = lax.all_gather(queries, Y, axis=0, tiled=True)
    f4, f8, f12 = (shifted(kv, "z", s) for s in (4, 8, -4))
    held = jnp.concatenate((kv, f4, f8, f12), axis=0)
    conv = jnp.concatenate((conv_weight, conv_bias[None, :]), axis=0)
    held, out_weight, residual, conv = lax.optimization_barrier(
        (held, out_weight, residual, conv)
    )
    out_weight, residual, conv = swapped(out_weight), swapped(residual), swapped(conv)
    n1 = shifted(held, "z", 1)
    n2a = shifted(held[: 2 * rows], "z", 2)
    back = jnp.concatenate((f12, kv), axis=0)
    n2b = shifted(back, "z", -2)
    n2 = jnp.concatenate((n2a, n2b), axis=0)
    n3 = shifted(jnp.concatenate((f4, f8, f12, kv), axis=0), "z", -1)
    far = held[rows:]
    parts = pl.pallas_call(
        attend_kernel,
        out_shape=jax.ShapeDtypeStruct((NY * rows, 3 * VD), jnp.bfloat16),
        in_specs=[SMEM] + [VMEM] * 6,
        out_specs=VMEM,
        name="attend",
    )(where, q_all, kv, far, n1, n2, n3)
    got = lax.all_to_all(parts.reshape(NY, rows, 3 * VD), Y, 0, 0, tiled=True)
    means = merged(got)
    diff = means[0] - second_weight[0] * means[1]
    scale_inv = lax.rsqrt(jnp.mean(diff * diff, axis=-1, keepdims=True) + eps)
    attended = swapped((diff * scale_inv * head_gain * 0.8).astype(jnp.bfloat16))
    proj = summed_over_shards(
        jnp.dot(attended, out_weight, preferred_element_type=jnp.float32).astype(jnp.bfloat16)
    )
    mid = (residual.astype(jnp.float32) + proj.astype(jnp.float32)).astype(jnp.bfloat16)
    normed = normalize(mid, norm_gain)
    mine, _ = lax.optimization_barrier((mine, normed))
    other = lax.ppermute(mine, "c", [(0, 1), (1, 0)])
    normed_all = lax.all_gather(normed, SHARDS, axis=0, tiled=True)
    tokens = ("z", "yh", "c")
    count = lax.axis_size(tokens)
    rim_rows = lax.ppermute(normed_all[rows - 8 :], tokens, [(i, i + 1) for i in range(count - 1)])
    normed_ext = jnp.concatenate((normed_all, rim_rows), axis=0)
    taps = conv_weight.shape[0]
    first, second = conv[:, :half], conv[:, half:]
    ffn = jnp.zeros((), jnp.float32)
    for w, units in (
        (mine, jnp.where(core == 0, first, second)),
        (other, jnp.where(core == 0, second, first)),
    ):
        both = jnp.dot(
            normed_ext, w[:, : 2 * half + gap], preferred_element_type=jnp.float32
        ).astype(jnp.bfloat16)
        up_proj, gate_proj = both[:rows, :half], both[:rows, half : 2 * half]
        extended = jnp.concatenate((both[rows + 8 - (taps - 1) :, :half], up_proj), axis=0)
        conv_out = jnp.zeros((rows, half), jnp.float32) + units[taps][None, :]
        for tap in range(taps):
            conv_out = conv_out + units[tap][None, :] * extended[tap : tap + rows].astype(
                jnp.float32
            )
        hidden = (jax.nn.silu(conv_out) * gate_proj.astype(jnp.float32)).astype(jnp.bfloat16)
        ffn = ffn + dot_nt(hidden, w[:, 2 * half + gap : width])
    ffn_out = summed_over_shards(ffn.astype(jnp.bfloat16))
    return swapped((mid.astype(jnp.float32) + ffn_out.astype(jnp.float32)).astype(jnp.bfloat16))


def solution(mesh):
    z = mesh.shape["sp"] // NY
    shape = (z, 2, 2, mesh.shape["tp"] // 2, 2)
    finer = Mesh(mesh.devices.reshape(shape), ("z", "yh", "yl", "x", "c"))
    in_specs = (
        P(SP + TP, None),
        P(SP, TP),
        P(SP, TP),
        P(SP, TP),
        P(TP),
        P(TP),
        P(TP, None),
        P(),
        P(SP, TP),
        P(SP, TP),
        P(None, TP),
        P(TP),
        P(TP, SP),
    )
    out_specs = P(SP + TP, None)
    return jax.shard_map(local, mesh=finer, in_specs=in_specs, out_specs=out_specs, check_vma=False)
```

```python
import jax
import jax.numpy as jnp
from jax import lax
from jax.experimental import pallas as pl
from jax.experimental.pallas import tpu as pltpu
from jax.sharding import Mesh
from jax.sharding import PartitionSpec as P

HD = 64
VD = 128
SP = ("z", "yh", "yl")
TP = ("x", "c")
Y = ("yh", "yl")
SHARDS = ("x", "yl")
NY = 4
LANES = 128
eps = 1e-05
neg_fill = -1e30
TILE = 128
FAR = (4, 8, 12)
NEAR = ((1, 5, 9, 13), (2, 6, 10, 14), (3, 7, 11, 15))

VMEM = pl.BlockSpec(memory_space=pltpu.VMEM)
SMEM = pl.BlockSpec(memory_space=pltpu.SMEM)


def shifted(value, axis, steps):
    count = lax.axis_size(axis)
    return lax.ppermute(value, axis, [(i, (i + steps) % count) for i in range(count)])


def swapped(value):
    return lax.ppermute(value, ("yl", "c"), [(0, 0), (1, 2), (2, 1), (3, 3)])


def dot_nt(a, b):
    return lax.dot_general(a, b, (((1,), (1,)), ((), ())), preferred_element_type=jnp.float32)


def attend_kernel(where_ref, rows_ref, own_ref, far_ref, n1_ref, n2_ref, n3_ref, out_ref, q_ref):
    z = where_ref[0]
    y = where_ref[1]
    rows = own_ref.shape[0]
    w_rows = rows_ref.shape[0] // NY
    for i in range(NY * rows // w_rows):
        y_at, lane_at = divmod(i, rows // w_rows)
        q_ref[i * w_rows : (i + 1) * w_rows, :] = rows_ref[
            y_at * w_rows : (y_at + 1) * w_rows, lane_at * 2 * HD : (lane_at + 1) * 2 * HD
        ]

    def row_bias(offsets):
        lane = lax.broadcasted_iota(jnp.int32, (1, rows * len(offsets)), 1)
        bias = jnp.zeros(lane.shape, jnp.float32)
        for i, off in enumerate(offsets):
            inside = jnp.logical_and(lane >= i * rows, lane < (i + 1) * rows)
            bias = jnp.where(jnp.logical_and(inside, off > z), neg_fill, bias)
        return bias

    pieces = ((far_ref, FAR), (n1_ref, NEAR[0]), (n2_ref, NEAR[1]), (n3_ref, NEAR[2]))
    biases = [row_bias(offsets) for _, offsets in pieces]
    lane_q = lax.broadcasted_iota(jnp.int32, (TILE, 2 * HD), 1)
    lane_s = lax.broadcasted_iota(jnp.int32, (TILE, VD), 1)

    @pl.loop(0, NY * rows // TILE)
    def _(t):
        at = pl.multiple_of(t * TILE, TILE)
        q = q_ref[pl.ds(at, TILE), :] * jnp.bfloat16(HD**-0.5)
        zero = jnp.zeros_like(q)
        q2 = jnp.concatenate(
            (jnp.where(lane_q < HD, q, zero), jnp.where(lane_q < HD, zero, q)), axis=0
        )
        s_own = dot_nt(q2, own_ref[:, : 2 * HD])
        r = lax.broadcasted_iota(jnp.int32, s_own.shape, 0)
        r = jnp.where(r >= TILE, r - TILE, r) + at
        k = lax.broadcasted_iota(jnp.int32, s_own.shape, 1) + y * rows
        s_own = jnp.where(k <= r, s_own, neg_fill)
        scores = [s_own] + [
            dot_nt(q2, ref[:, : 2 * HD]) + bias for (ref, _), bias in zip(pieces, biases)
        ]
        top = jnp.max(scores[0], axis=1, keepdims=True)
        for s in scores[1:]:
            top = jnp.maximum(top, jnp.max(s, axis=1, keepdims=True))
        total = jnp.zeros((2 * TILE, 1), jnp.float32)
        acc = jnp.zeros((2 * TILE, VD), jnp.float32)
        for s, ref in zip(scores, (own_ref, far_ref, n1_ref, n2_ref, n3_ref)):
            e = jnp.exp(s - top)
            total = total + jnp.sum(e, axis=1, keepdims=True)
            acc = acc + jnp.dot(
                e.astype(jnp.bfloat16), ref[:, 2 * HD :], preferred_element_type=jnp.float32
            )
        mean = acc / total
        lse = top + jnp.log(total)
        hi = lse.astype(jnp.bfloat16).astype(jnp.float32)
        mid = (lse - hi).astype(jnp.bfloat16).astype(jnp.float32)
        low = lse - hi - mid
        stat = jnp.zeros((TILE, VD), jnp.float32)
        for m in range(2):
            for i, v in enumerate((hi, mid, low)):
                stat = jnp.where(lane_s == 3 * m + i, v[m * TILE : (m + 1) * TILE], stat)
        out_ref[pl.ds(at, TILE), 0:VD] = mean[:TILE].astype(jnp.bfloat16)
        out_ref[pl.ds(at, TILE), VD : 2 * VD] = mean[TILE:].astype(jnp.bfloat16)
        out_ref[pl.ds(at, TILE), 2 * VD : 3 * VD] = stat.astype(jnp.bfloat16)


def merged(got):
    got = got.astype(jnp.float32)
    means = []
    for m in range(2):
        stat = got[:, :, 2 * VD + 3 * m : 2 * VD + 3 * m + 3]
        lse = stat[..., 0:1] + stat[..., 1:2] + stat[..., 2:3]
        share = jnp.exp(lse - jnp.max(lse, axis=0, keepdims=True))
        acc = jnp.sum(share * got[:, :, m * VD : (m + 1) * VD], axis=0)
        means.append(acc / jnp.sum(share, axis=0))
    return means


def normalize(rows_in, gain):
    values_f = rows_in.astype(jnp.float32)
    scale_inv = lax.rsqrt(jnp.mean(values_f * values_f, axis=-1, keepdims=True) + eps)
    return (values_f * scale_inv * gain).astype(jnp.bfloat16)


def summed_over_shards(shard):
    count = lax.axis_size(SHARDS)
    cut = shard.reshape(count, shard.shape[0] // count, shard.shape[1])
    tiles = lax.all_to_all(cut, SHARDS, 0, 0, tiled=True)
    return jnp.sum(tiles.astype(jnp.float32), axis=0).astype(jnp.bfloat16)


def local(
    residual,
    queries,
    key_pairs,
    values,
    second_weight,
    head_gain,
    out_weight,
    norm_gain,
    up_weight,
    gate_weight,
    conv_weight,
    conv_bias,
    down_weight,
):
    rows = queries.shape[0]
    ff = up_weight.shape[1]
    half = ff // 2
    core = lax.axis_index("c")
    pair = lax.axis_index("yl")
    y_index = lax.axis_index("yh") * 2 + pair
    where = jnp.stack((lax.axis_index("z"), y_index)).astype(jnp.int32)

    down_t = down_weight.T
    gap = -2 * half % LANES
    width = 2 * half + gap + half
    tail = -width % LANES
    cuts = []
    for h in range(2):
        units = slice(h * half, (h + 1) * half)
        cuts += [up_weight[:, units], gate_weight[:, units]]
        cuts += [jnp.zeros((up_weight.shape[0], gap), jnp.bfloat16), down_t[:, units]]
        cuts += [jnp.zeros((up_weight.shape[0], tail), jnp.bfloat16)]
    w_rows = up_weight.shape[0]
    cuts += [queries[i : i + w_rows] for i in range(0, rows, w_rows)]
    row_w = lax.all_gather(jnp.concatenate(cuts, axis=1), Y, axis=0, tiled=True)
    span = width + tail
    low, high = row_w[:, :span], row_w[:, span : 2 * span]
    q_rows = row_w[:, 2 * span :]
    for_peer = lax.ppermute(jnp.where(core == 0, high, low), ("yl", "c"), [(0, 1), (3, 2)])
    kept = jnp.where(core == pair, jnp.where(core == 0, low, high), for_peer)
    mine = lax.all_gather(kept, "z", axis=0, tiled=True)

    kv = jnp.concatenate((key_pairs, values), axis=1)
    f4, f8, f12 = (shifted(kv, "z", s) for s in (4, 8, -4))
    held = jnp.concatenate((kv, f4, f8, f12), axis=0)
    conv = jnp.concatenate((conv_weight, conv_bias[None, :]), axis=0)
    held, out_weight, residual, conv = lax.optimization_barrier(
        (held, out_weight, residual, conv)
    )
    out_weight, residual, conv = swapped(out_weight), swapped(residual), swapped(conv)
    n1 = shifted(held, "z", 1)
    n2a = shifted(held[: 2 * rows], "z", 2)
    back = jnp.concatenate((f12, kv), axis=0)
    n2b = shifted(back, "z", -2)
    n2 = jnp.concatenate((n2a, n2b), axis=0)
    n3 = shifted(jnp.concatenate((f4, f8, f12, kv), axis=0), "z", -1)
    far = held[rows:]
    parts = pl.pallas_call(
        attend_kernel,
        out_shape=jax.ShapeDtypeStruct((NY * rows, 3 * VD), jnp.bfloat16),
        in_specs=[SMEM] + [VMEM] * 6,
        out_specs=VMEM,
        scratch_shapes=[pltpu.VMEM((NY * rows, 2 * HD), jnp.bfloat16)],
        name="attend",
    )(where, q_rows, kv, far, n1, n2, n3)
    got = lax.all_to_all(parts.reshape(NY, rows, 3 * VD), Y, 0, 0, tiled=True)
    means = merged(got)
    diff = means[0] - second_weight[0] * means[1]
    scale_inv = lax.rsqrt(jnp.mean(diff * diff, axis=-1, keepdims=True) + eps)
    attended = swapped((diff * scale_inv * head_gain * 0.8).astype(jnp.bfloat16))
    proj = summed_over_shards(
        jnp.dot(attended, out_weight, preferred_element_type=jnp.float32).astype(jnp.bfloat16)
    )
    mid = (residual.astype(jnp.float32) + proj.astype(jnp.float32)).astype(jnp.bfloat16)
    normed = normalize(mid, norm_gain)
    mine, _ = lax.optimization_barrier((mine, normed))
    other = lax.ppermute(mine, "c", [(0, 1), (1, 0)])
    peer = lax.ppermute(normed, "yl", [(0, 1), (1, 0)])
    both_rows = jnp.concatenate(
        (jnp.where(pair == 0, normed, peer), jnp.where(pair == 0, peer, normed)), axis=0
    )
    normed_all = lax.all_gather(both_rows, "x", axis=0, tiled=True)
    tokens = ("z", "yh", "c")
    count = lax.axis_size(tokens)
    rim_rows = lax.ppermute(normed_all[rows - 8 :], tokens, [(i, i + 1) for i in range(count - 1)])
    normed_ext = jnp.concatenate((normed_all, rim_rows), axis=0)
    taps = conv_weight.shape[0]
    first, second = conv[:, :half], conv[:, half:]
    ffn = jnp.zeros((), jnp.float32)
    for w, units in (
        (mine, jnp.where(core == 0, first, second)),
        (other, jnp.where(core == 0, second, first)),
    ):
        both = jnp.dot(
            normed_ext, w[:, : 2 * half + gap], preferred_element_type=jnp.float32
        ).astype(jnp.bfloat16)
        up_proj, gate_proj = both[:rows, :half], both[:rows, half : 2 * half]
        extended = jnp.concatenate((both[rows + 8 - (taps - 1) :, :half], up_proj), axis=0)
        conv_out = jnp.zeros((rows, half), jnp.float32) + units[taps][None, :]
        for tap in range(taps):
            conv_out = conv_out + units[tap][None, :] * extended[tap : tap + rows].astype(
                jnp.float32
            )
        hidden = (jax.nn.silu(conv_out) * gate_proj.astype(jnp.float32)).astype(jnp.bfloat16)
        ffn = ffn + dot_nt(hidden, w[:, 2 * half + gap : width])
    ffn_out = summed_over_shards(ffn.astype(jnp.bfloat16))
    return swapped((mid.astype(jnp.float32) + ffn_out.astype(jnp.float32)).astype(jnp.bfloat16))


def solution(mesh):
    z = mesh.shape["sp"] // NY
    shape = (z, 2, 2, mesh.shape["tp"] // 2, 2)
    finer = Mesh(mesh.devices.reshape(shape), ("z", "yh", "yl", "x", "c"))
    in_specs = (
        P(SP + TP, None),
        P(SP, TP),
        P(SP, TP),
        P(SP, TP),
        P(TP),
        P(TP),
        P(TP, None),
        P(),
        P(SP, TP),
        P(SP, TP),
        P(None, TP),
        P(TP),
        P(TP, SP),
    )
    out_specs = P(SP + TP, None)
    return jax.shard_map(local, mesh=finer, in_specs=in_specs, out_specs=out_specs, check_vma=False)
```

```python
import jax
import jax.numpy as jnp
from jax import lax
from jax.experimental import pallas as pl
from jax.experimental.pallas import tpu as pltpu
from jax.sharding import Mesh
from jax.sharding import PartitionSpec as P

HD = 64
VD = 128
SP = ("z", "y")
SP_TP = ("z", "y", "tp")
NZ = 16
NY = 4
eps = 1e-05
neg_fill = -1e30
TILE = 128
LANES = 128
EARLY = ((5, 11), (1, 6, 12), (15, 4, 10))
LATE = ((8,), (2, 7, 13), (14, 3, 9))

VMEM = pl.BlockSpec(memory_space=pltpu.VMEM)
SMEM = pl.BlockSpec(memory_space=pltpu.SMEM)


def shifted(value, axis, steps):
    count = lax.axis_size(axis)
    return lax.ppermute(value, axis, [(i, (i + steps) % count) for i in range(count)])


def dot_nt(a, b):
    return lax.dot_general(a, b, (((1,), (1,)), ((), ())), preferred_element_type=jnp.float32)


def row_bias(offsets, rows, z):
    lane = lax.broadcasted_iota(jnp.int32, (1, rows * len(offsets)), 1)
    bias = jnp.zeros(lane.shape, jnp.float32)
    for i, off in enumerate(offsets):
        inside = jnp.logical_and(lane >= i * rows, lane < (i + 1) * rows)
        bias = jnp.where(jnp.logical_and(inside, off > z), neg_fill, bias)
    return bias


def both_maps(q):
    lane = lax.broadcasted_iota(jnp.int32, q.shape, 1)
    q = q * jnp.bfloat16(HD**-0.5)
    zero = jnp.zeros_like(q)
    return jnp.concatenate((jnp.where(lane < HD, q, zero), jnp.where(lane < HD, zero, q)), axis=0)


def softmax_step(scores, refs, top, total, acc):
    new_top = top
    for s in scores:
        new_top = jnp.maximum(new_top, jnp.max(s, axis=1, keepdims=True))
    keep = jnp.exp(top - new_top)
    total = total * keep
    acc = acc * keep
    for s, ref in zip(scores, refs):
        e = jnp.exp(s - new_top)
        total = total + jnp.sum(e, axis=1, keepdims=True)
        acc = acc + jnp.dot(
            e.astype(jnp.bfloat16), ref[:, 2 * HD :], preferred_element_type=jnp.float32
        )
    return new_top, total, acc


def packed(columns):
    lane = lax.broadcasted_iota(jnp.int32, (TILE, VD), 1)
    block = jnp.zeros((TILE, VD), jnp.float32)
    for m in range(2):
        for i, v in enumerate(columns):
            column = v[m * TILE : (m + 1) * TILE]
            block = jnp.where(lane == m * len(columns) + i, column, block)
    return block


def early_kernel(where_ref, rows_ref, held_ref, n1_ref, m1_ref, state_ref, q_ref):
    z = where_ref[0]
    y = where_ref[1]
    rows = held_ref.shape[0] // 3
    own_ref, far_ref = held_ref.at[0:rows], held_ref.at[rows:]
    w_rows = rows_ref.shape[0] // NY
    for i in range(NY * rows // w_rows):
        y_at, lane_at = divmod(i, rows // w_rows)
        q_ref[i * w_rows : (i + 1) * w_rows, :] = rows_ref[
            y_at * w_rows : (y_at + 1) * w_rows, lane_at * 2 * HD : (lane_at + 1) * 2 * HD
        ]
    refs = (far_ref, n1_ref, m1_ref)
    biases = [row_bias(offsets, rows, z) for offsets in EARLY]

    @pl.loop(0, NY * rows // TILE)
    def _(t):
        at = pl.multiple_of(t * TILE, TILE)
        q2 = both_maps(q_ref[pl.ds(at, TILE), :])
        s_own = dot_nt(q2, own_ref[:, : 2 * HD])
        r = lax.broadcasted_iota(jnp.int32, s_own.shape, 0)
        r = jnp.where(r >= TILE, r - TILE, r) + at
        k = lax.broadcasted_iota(jnp.int32, s_own.shape, 1) + y * rows
        s_own = jnp.where(k <= r, s_own, neg_fill)
        scores = [s_own] + [dot_nt(q2, ref[:, : 2 * HD]) + b for ref, b in zip(refs, biases)]
        top = jnp.full((2 * TILE, 1), neg_fill, jnp.float32)
        zero = jnp.zeros((2 * TILE, 1), jnp.float32)
        acc = jnp.zeros((2 * TILE, VD), jnp.float32)
        top, total, acc = softmax_step(scores, (own_ref, *refs), top, zero, acc)
        state_ref[pl.ds(at, TILE), 0:VD] = acc[:TILE]
        state_ref[pl.ds(at, TILE), VD : 2 * VD] = acc[TILE:]
        state_ref[pl.ds(at, TILE), 2 * VD : 3 * VD] = packed((top, total))


def late_kernel(where_ref, q_ref, state_ref, e8_ref, n2_ref, m2_ref, out_ref):
    z = where_ref[0]
    refs = (e8_ref, n2_ref, m2_ref)
    rows = e8_ref.shape[0]
    biases = [row_bias(offsets, rows, z) for offsets in LATE]

    @pl.loop(0, NY * rows // TILE)
    def _(t):
        at = pl.multiple_of(t * TILE, TILE)
        q2 = both_maps(q_ref[pl.ds(at, TILE), :])
        scores = [dot_nt(q2, ref[:, : 2 * HD]) + b for ref, b in zip(refs, biases)]
        stat = state_ref[pl.ds(at, TILE), 2 * VD : 3 * VD]
        top = jnp.concatenate((stat[:, 0:1], stat[:, 2:3]), axis=0)
        total = jnp.concatenate((stat[:, 1:2], stat[:, 3:4]), axis=0)
        acc = jnp.concatenate(
            (state_ref[pl.ds(at, TILE), 0:VD], state_ref[pl.ds(at, TILE), VD : 2 * VD]), axis=0
        )
        top, total, acc = softmax_step(scores, refs, top, total, acc)
        mean = acc / total
        lse = top + jnp.log(total)
        hi = lse.astype(jnp.bfloat16).astype(jnp.float32)
        mid = (lse - hi).astype(jnp.bfloat16).astype(jnp.float32)
        out_ref[pl.ds(at, TILE), 0:VD] = mean[:TILE].astype(jnp.bfloat16)
        out_ref[pl.ds(at, TILE), VD : 2 * VD] = mean[TILE:].astype(jnp.bfloat16)
        out_ref[pl.ds(at, TILE), 2 * VD : 3 * VD] = packed((hi, mid, lse - hi - mid)).astype(
            jnp.bfloat16
        )


def merged(got):
    got = got.astype(jnp.float32)
    means = []
    for m in range(2):
        stat = got[:, :, 2 * VD + 3 * m : 2 * VD + 3 * m + 3]
        lse = stat[..., 0:1] + stat[..., 1:2] + stat[..., 2:3]
        share = jnp.exp(lse - jnp.max(lse, axis=0, keepdims=True))
        acc = jnp.sum(share * got[:, :, m * VD : (m + 1) * VD], axis=0)
        means.append(acc / jnp.sum(share, axis=0))
    return means


def normalize(rows_in, gain):
    values_f = rows_in.astype(jnp.float32)
    scale_inv = lax.rsqrt(jnp.mean(values_f * values_f, axis=-1, keepdims=True) + eps)
    return (values_f * scale_inv * gain).astype(jnp.bfloat16)


def summed_over_tp(shard):
    count = lax.axis_size("tp")
    cut = shard.reshape(count, shard.shape[0] // count, shard.shape[1])
    tiles = lax.all_to_all(cut, "tp", 0, 0, tiled=True)
    return jnp.sum(tiles.astype(jnp.float32), axis=0).astype(jnp.bfloat16)


def local(
    residual,
    queries,
    key_pairs,
    values,
    second_weight,
    head_gain,
    out_weight,
    norm_gain,
    up_weight,
    gate_weight,
    conv_weight,
    conv_bias,
    down_weight,
):
    rows = queries.shape[0]
    ff = up_weight.shape[1]
    where = jnp.stack((lax.axis_index("z"), lax.axis_index("y"))).astype(jnp.int32)
    w_rows = up_weight.shape[0]
    width = 2 * ff + ff
    tail = -width % LANES
    cuts = [up_weight, gate_weight, down_weight.T, jnp.zeros((w_rows, tail), jnp.bfloat16)]
    cuts += [queries[i : i + w_rows] for i in range(0, rows, w_rows)]
    row_w = lax.all_gather(jnp.concatenate(cuts, axis=1), "y", axis=0, tiled=True)
    all_w = lax.all_gather(row_w[:, :width], "z", axis=0, tiled=True)
    q_rows = row_w[:, width + tail :]

    kv = jnp.concatenate((key_pairs, values), axis=1)
    f5, f11 = shifted(kv, "z", 5), shifted(kv, "z", -5)
    held = jnp.concatenate((kv, f5, f11), axis=0)
    n1 = shifted(held, "z", 1)
    m1 = shifted(held, "z", -1)
    e8 = shifted(f5, "z", 3)
    n2 = shifted(n1, "z", 1)
    m2 = shifted(m1, "z", -1)
    state, q_all = pl.pallas_call(
        early_kernel,
        out_shape=[
            jax.ShapeDtypeStruct((NY * rows, 3 * VD), jnp.float32),
            jax.ShapeDtypeStruct((NY * rows, 2 * HD), jnp.bfloat16),
        ],
        in_specs=[SMEM] + [VMEM] * 4,
        out_specs=[VMEM] * 2,
        name="early",
    )(where, q_rows, held, n1, m1)
    parts = pl.pallas_call(
        late_kernel,
        out_shape=jax.ShapeDtypeStruct((NY * rows, 3 * VD), jnp.bfloat16),
        in_specs=[SMEM] + [VMEM] * 5,
        out_specs=VMEM,
        name="late",
    )(where, q_all, state, e8, n2, m2)
    got = lax.all_to_all(parts.reshape(NY, rows, 3 * VD), "y", 0, 0, tiled=True)
    means = merged(got)
    diff = means[0] - second_weight[0] * means[1]
    scale_inv = lax.rsqrt(jnp.mean(diff * diff, axis=-1, keepdims=True) + eps)
    attended = (diff * scale_inv * head_gain * 0.8).astype(jnp.bfloat16)
    proj = summed_over_tp(
        jnp.dot(attended, out_weight, preferred_element_type=jnp.float32).astype(jnp.bfloat16)
    )
    mid = (residual.astype(jnp.float32) + proj.astype(jnp.float32)).astype(jnp.bfloat16)
    normed_all = lax.all_gather(normalize(mid, norm_gain), "tp", axis=0, tiled=True)
    count = lax.axis_size("z") * lax.axis_size("y")
    rim_rows = lax.ppermute(normed_all[rows - 8 :], SP, [(i, i + 1) for i in range(count - 1)])
    both = jnp.dot(
        jnp.concatenate((normed_all, rim_rows), axis=0),
        all_w[:, : 2 * ff],
        preferred_element_type=jnp.float32,
    ).astype(jnp.bfloat16)
    up_proj, gate_proj = both[:rows, :ff], both[:rows, ff:]
    taps = conv_weight.shape[0]
    extended = jnp.concatenate((both[rows + 8 - (taps - 1) :, :ff], up_proj), axis=0)
    conv_out = jnp.zeros((rows, ff), jnp.float32) + conv_bias[None, :]
    for tap in range(taps):
        conv_out = conv_out + conv_weight[tap][None, :] * extended[tap : tap + rows].astype(
            jnp.float32
        )
    hidden = (jax.nn.silu(conv_out) * gate_proj.astype(jnp.float32)).astype(jnp.bfloat16)
    ffn = dot_nt(hidden, all_w[:, 2 * ff : width]).astype(jnp.bfloat16)
    ffn_out = summed_over_tp(ffn)
    return (mid.astype(jnp.float32) + ffn_out.astype(jnp.float32)).astype(jnp.bfloat16)


def solution(mesh):
    finer = Mesh(mesh.devices.reshape(NZ, NY, mesh.shape["tp"]), ("z", "y", "tp"))
    in_specs = (
        P(SP_TP, None),
        P(SP, "tp"),
        P(SP, "tp"),
        P(SP, "tp"),
        P("tp"),
        P("tp"),
        P("tp", None),
        P(),
        P(SP, "tp"),
        P(SP, "tp"),
        P(None, "tp"),
        P("tp"),
        P("tp", SP),
    )
    out_specs = P(SP_TP, None)
    return jax.shard_map(local, mesh=finer, in_specs=in_specs, out_specs=out_specs, check_vma=False)
```

```python
import jax
import jax.numpy as jnp
from jax import lax
from jax.experimental import pallas as pl
from jax.experimental.pallas import tpu as pltpu
from jax.sharding import Mesh
from jax.sharding import PartitionSpec as P

HD = 64
VD = 128
SP = ("z", "y")
SP_TP = ("z", "y", "x", "c")
TP = ("x", "c")
NZ = 16
NY = 4
eps = 1e-05
neg_fill = -1e30
TILE = 128
LANES = 128
OFFSETS = (0, 1, 15, 2, 14, 3, 13, 4, 12, 5, 11, 6, 10, 7, 9, 8)
CHUNK = 4

VMEM = pl.BlockSpec(memory_space=pltpu.VMEM)
SMEM = pl.BlockSpec(memory_space=pltpu.SMEM)


def shifted(value, axis, steps):
    count = lax.axis_size(axis)
    return lax.ppermute(value, axis, [(i, (i + steps) % count) for i in range(count)])


def dot_nt(a, b):
    return lax.dot_general(a, b, (((1,), (1,)), ((), ())), preferred_element_type=jnp.float32)


def row_bias(offsets, rows, z):
    lane = lax.broadcasted_iota(jnp.int32, (1, rows * len(offsets)), 1)
    bias = jnp.zeros(lane.shape, jnp.float32)
    for i, off in enumerate(offsets):
        inside = jnp.logical_and(lane >= i * rows, lane < (i + 1) * rows)
        bias = jnp.where(jnp.logical_and(inside, off > z), neg_fill, bias)
    return bias


def both_maps(q):
    lane = lax.broadcasted_iota(jnp.int32, q.shape, 1)
    q = q * jnp.bfloat16(HD**-0.5)
    zero = jnp.zeros_like(q)
    return jnp.concatenate((jnp.where(lane < HD, q, zero), jnp.where(lane < HD, zero, q)), axis=0)


def packed(columns):
    lane = lax.broadcasted_iota(jnp.int32, (TILE, VD), 1)
    block = jnp.zeros((TILE, VD), jnp.float32)
    for m in range(2):
        for i, v in enumerate(columns):
            column = v[m * TILE : (m + 1) * TILE]
            block = jnp.where(lane == m * len(columns) + i, column, block)
    return block


def attend_kernel(where_ref, rows_ref, *refs):
    blocks, (out_ref, q_ref, kv_ref) = refs[:-3], refs[-3:]
    z = where_ref[0]
    y = where_ref[1]
    rows = blocks[0].shape[0]
    w_rows = rows_ref.shape[0] // NY
    for i in range(NY * rows // w_rows):
        y_at, lane_at = divmod(i, rows // w_rows)
        q_ref[i * w_rows : (i + 1) * w_rows, :] = rows_ref[
            y_at * w_rows : (y_at + 1) * w_rows, lane_at * 2 * HD : (lane_at + 1) * 2 * HD
        ]
    for i, block in enumerate(blocks):
        kv_ref[i * rows : (i + 1) * rows, :] = block[...]
    span = CHUNK * rows
    chunks = [OFFSETS[i : i + CHUNK] for i in range(0, len(OFFSETS), CHUNK)]
    biases = [row_bias(offsets, rows, z) for offsets in chunks]

    @pl.loop(0, NY * rows // TILE)
    def _(t):
        at = pl.multiple_of(t * TILE, TILE)
        q2 = both_maps(q_ref[pl.ds(at, TILE), :])
        scores = []
        for i, bias in enumerate(biases):
            keys = kv_ref[i * span : (i + 1) * span, : 2 * HD]
            scores.append(dot_nt(q2, keys) + bias)
        r = lax.broadcasted_iota(jnp.int32, scores[0].shape, 0)
        r = jnp.where(r >= TILE, r - TILE, r) + at
        k = lax.broadcasted_iota(jnp.int32, scores[0].shape, 1)
        hidden = jnp.logical_and(k < rows, k + y * rows > r)
        scores[0] = jnp.where(hidden, neg_fill, scores[0])
        top = jnp.max(scores[0], axis=1, keepdims=True)
        for s in scores[1:]:
            top = jnp.maximum(top, jnp.max(s, axis=1, keepdims=True))
        total = jnp.zeros((2 * TILE, 1), jnp.float32)
        acc = jnp.zeros((2 * TILE, VD), jnp.float32)
        for i, s in enumerate(scores):
            e = jnp.exp(s - top)
            total = total + jnp.sum(e, axis=1, keepdims=True)
            acc = acc + jnp.dot(
                e.astype(jnp.bfloat16),
                kv_ref[i * span : (i + 1) * span, 2 * HD :],
                preferred_element_type=jnp.float32,
            )
        mean = acc / total
        lse = top + jnp.log(total)
        hi = lse.astype(jnp.bfloat16).astype(jnp.float32)
        mid = (lse - hi).astype(jnp.bfloat16).astype(jnp.float32)
        out_ref[pl.ds(at, TILE), 0:VD] = mean[:TILE].astype(jnp.bfloat16)
        out_ref[pl.ds(at, TILE), VD : 2 * VD] = mean[TILE:].astype(jnp.bfloat16)
        out_ref[pl.ds(at, TILE), 2 * VD : 3 * VD] = packed((hi, mid, lse - hi - mid)).astype(
            jnp.bfloat16
        )


def merged(got):
    got = got.astype(jnp.float32)
    means = []
    for m in range(2):
        stat = got[:, :, 2 * VD + 3 * m : 2 * VD + 3 * m + 3]
        lse = stat[..., 0:1] + stat[..., 1:2] + stat[..., 2:3]
        share = jnp.exp(lse - jnp.max(lse, axis=0, keepdims=True))
        acc = jnp.sum(share * got[:, :, m * VD : (m + 1) * VD], axis=0)
        means.append(acc / jnp.sum(share, axis=0))
    return means


def normalize(rows_in, gain):
    values_f = rows_in.astype(jnp.float32)
    scale_inv = lax.rsqrt(jnp.mean(values_f * values_f, axis=-1, keepdims=True) + eps)
    return (values_f * scale_inv * gain).astype(jnp.bfloat16)


def summed_over_tp(shard):
    core = lax.axis_index("c")
    count = lax.axis_size(TP)
    cut = shard.reshape(count // 2, 2, shard.shape[0] // count, shard.shape[1])
    own = jnp.where(core == 0, cut[:, 0], cut[:, 1])
    for_peer = jnp.where(core == 0, cut[:, 1], cut[:, 0])
    from_peer = lax.ppermute(for_peer, "c", [(0, 1), (1, 0)])
    both = (own.astype(jnp.float32) + from_peer.astype(jnp.float32)).astype(jnp.bfloat16)
    tiles = lax.all_to_all(both, "x", 0, 0, tiled=True)
    return jnp.sum(tiles.astype(jnp.float32), axis=0).astype(jnp.bfloat16)


def local(
    residual,
    queries,
    key_pairs,
    values,
    second_weight,
    head_gain,
    out_weight,
    norm_gain,
    up_weight,
    gate_weight,
    conv_weight,
    conv_bias,
    down_weight,
):
    rows = queries.shape[0]
    ff = up_weight.shape[1]
    where = jnp.stack((lax.axis_index("z"), lax.axis_index("y"))).astype(jnp.int32)
    w_rows = up_weight.shape[0]
    width = 2 * ff + ff
    tail = -width % LANES
    cuts = [up_weight, gate_weight, down_weight.T, jnp.zeros((w_rows, tail), jnp.bfloat16)]
    cuts += [queries[i : i + w_rows] for i in range(0, rows, w_rows)]
    row_w = lax.all_gather(jnp.concatenate(cuts, axis=1), "y", axis=0, tiled=True)
    all_w = lax.all_gather(row_w[:, :width], "z", axis=0, tiled=True)
    q_rows = row_w[:, width + tail :]

    kv = jnp.concatenate((key_pairs, values), axis=1)
    ahead, behind, blocks = kv, kv, [kv]
    for _ in range(lax.axis_size("z") // 2 - 1):
        ahead, behind = shifted(ahead, "z", 1), shifted(behind, "z", -1)
        blocks += [ahead, behind]
    cut = rows // 2
    far = (shifted(ahead[:cut], "z", 1), shifted(behind[cut:], "z", -1))
    blocks.append(jnp.concatenate(far, axis=0))
    blocks = [pltpu.with_memory_space_constraint(b, pltpu.VMEM) for b in blocks]
    parts = pl.pallas_call(
        attend_kernel,
        out_shape=jax.ShapeDtypeStruct((NY * rows, 3 * VD), jnp.bfloat16),
        in_specs=[SMEM] + [VMEM] * (1 + len(blocks)),
        out_specs=VMEM,
        scratch_shapes=[
            pltpu.VMEM((NY * rows, 2 * HD), jnp.bfloat16),
            pltpu.VMEM((len(blocks) * rows, 2 * HD + VD), jnp.bfloat16),
        ],
        name="attend",
    )(where, q_rows, *blocks)
    got = lax.all_to_all(parts.reshape(NY, rows, 3 * VD), "y", 0, 0, tiled=True)
    means = merged(got)
    diff = means[0] - second_weight[0] * means[1]
    scale_inv = lax.rsqrt(jnp.mean(diff * diff, axis=-1, keepdims=True) + eps)
    attended = (diff * scale_inv * head_gain * 0.8).astype(jnp.bfloat16)
    proj = summed_over_tp(
        jnp.dot(attended, out_weight, preferred_element_type=jnp.float32).astype(jnp.bfloat16)
    )
    mid = (residual.astype(jnp.float32) + proj.astype(jnp.float32)).astype(jnp.bfloat16)
    normed_all = lax.all_gather(normalize(mid, norm_gain), TP, axis=0, tiled=True)
    count = lax.axis_size("z") * lax.axis_size("y")
    rim_rows = lax.ppermute(normed_all[rows - 8 :], SP, [(i, i + 1) for i in range(count - 1)])
    both = jnp.dot(
        jnp.concatenate((normed_all, rim_rows), axis=0),
        all_w[:, : 2 * ff],
        preferred_element_type=jnp.float32,
    ).astype(jnp.bfloat16)
    up_proj, gate_proj = both[:rows, :ff], both[:rows, ff:]
    taps = conv_weight.shape[0]
    extended = jnp.concatenate((both[rows + 8 - (taps - 1) :, :ff], up_proj), axis=0)
    conv_out = jnp.zeros((rows, ff), jnp.float32) + conv_bias[None, :]
    for tap in range(taps):
        conv_out = conv_out + conv_weight[tap][None, :] * extended[tap : tap + rows].astype(
            jnp.float32
        )
    hidden = (jax.nn.silu(conv_out) * gate_proj.astype(jnp.float32)).astype(jnp.bfloat16)
    ffn = dot_nt(hidden, all_w[:, 2 * ff : width]).astype(jnp.bfloat16)
    ffn_out = summed_over_tp(ffn)
    return (mid.astype(jnp.float32) + ffn_out.astype(jnp.float32)).astype(jnp.bfloat16)


def solution(mesh):
    finer = Mesh(mesh.devices.reshape(NZ, NY, mesh.shape["tp"] // 2, 2), ("z", "y", "x", "c"))
    in_specs = (
        P(SP_TP, None),
        P(SP, TP),
        P(SP, TP),
        P(SP, TP),
        P(TP),
        P(TP),
        P(TP, None),
        P(),
        P(SP, TP),
        P(SP, TP),
        P(None, TP),
        P(TP),
        P(TP, SP),
    )
    out_specs = P(SP_TP, None)
    return jax.shard_map(local, mesh=finer, in_specs=in_specs, out_specs=out_specs, check_vma=False)
```

```python
import jax
import jax.numpy as jnp
from jax import lax
from jax.experimental import pallas as pl
from jax.experimental.pallas import tpu as pltpu
from jax.sharding import Mesh
from jax.sharding import PartitionSpec as P

HD = 64
VD = 128
SP = ("z", "y")
SP_TP = ("z", "y", "x", "c")
TP = ("x", "c")
NZ = 16
NY = 4
eps = 1e-05
neg_fill = -1e30
TILE = 128
LANES = 128
OFFSETS = (0, 5, 11, 1, 6, 12, 15, 4, 10, 2, 7, 13, 14, 3, 9, 8)
CHUNK = 4

VMEM = pl.BlockSpec(memory_space=pltpu.VMEM)
SMEM = pl.BlockSpec(memory_space=pltpu.SMEM)


def shifted(value, steps, targets):
    count = lax.axis_size("z")
    return lax.ppermute(value, "z", [((i - steps) % count, i) for i in targets])


def dot_nt(a, b):
    return lax.dot_general(a, b, (((1,), (1,)), ((), ())), preferred_element_type=jnp.float32)


def row_bias(offsets, rows, z):
    lane = lax.broadcasted_iota(jnp.int32, (1, rows * len(offsets)), 1)
    bias = jnp.zeros(lane.shape, jnp.float32)
    for i, off in enumerate(offsets):
        inside = jnp.logical_and(lane >= i * rows, lane < (i + 1) * rows)
        bias = jnp.where(jnp.logical_and(inside, off > z), neg_fill, bias)
    return bias


def both_maps(q):
    lane = lax.broadcasted_iota(jnp.int32, q.shape, 1)
    q = q * jnp.bfloat16(HD**-0.5)
    zero = jnp.zeros_like(q)
    return jnp.concatenate((jnp.where(lane < HD, q, zero), jnp.where(lane < HD, zero, q)), axis=0)


def packed(columns):
    lane = lax.broadcasted_iota(jnp.int32, (TILE, VD), 1)
    block = jnp.zeros((TILE, VD), jnp.float32)
    for m in range(2):
        for i, v in enumerate(columns):
            column = v[m * TILE : (m + 1) * TILE]
            block = jnp.where(lane == m * len(columns) + i, column, block)
    return block


def attend_kernel(where_ref, rows_ref, *refs):
    blocks, (out_ref, q_ref, kv_ref) = refs[:-3], refs[-3:]
    z = where_ref[0]
    y = where_ref[1]
    rows = kv_ref.shape[0] // len(OFFSETS)
    w_rows = rows_ref.shape[0] // NY
    for i in range(NY * rows // w_rows):
        y_at, lane_at = divmod(i, rows // w_rows)
        q_ref[i * w_rows : (i + 1) * w_rows, :] = rows_ref[
            y_at * w_rows : (y_at + 1) * w_rows, lane_at * 2 * HD : (lane_at + 1) * 2 * HD
        ]
    filled = 0
    for block in blocks:
        kv_ref[filled : filled + block.shape[0], :] = block[...]
        filled += block.shape[0]
    span = CHUNK * rows
    chunks = [OFFSETS[i : i + CHUNK] for i in range(0, len(OFFSETS), CHUNK)]
    biases = [row_bias(offsets, rows, z) for offsets in chunks]

    @pl.loop(0, NY * rows // TILE)
    def _(t):
        at = pl.multiple_of(t * TILE, TILE)
        q2 = both_maps(q_ref[pl.ds(at, TILE), :])
        scores = []
        for i, bias in enumerate(biases):
            keys = kv_ref[i * span : (i + 1) * span, : 2 * HD]
            scores.append(dot_nt(q2, keys) + bias)
        r = lax.broadcasted_iota(jnp.int32, scores[0].shape, 0)
        r = jnp.where(r >= TILE, r - TILE, r) + at
        k = lax.broadcasted_iota(jnp.int32, scores[0].shape, 1)
        hidden = jnp.logical_and(k < rows, k + y * rows > r)
        scores[0] = jnp.where(hidden, neg_fill, scores[0])
        top = jnp.max(scores[0], axis=1, keepdims=True)
        for s in scores[1:]:
            top = jnp.maximum(top, jnp.max(s, axis=1, keepdims=True))
        total = jnp.zeros((2 * TILE, 1), jnp.float32)
        acc = jnp.zeros((2 * TILE, VD), jnp.float32)
        for i, s in enumerate(scores):
            e = jnp.exp(s - top)
            total = total + jnp.sum(e, axis=1, keepdims=True)
            acc = acc + jnp.dot(
                e.astype(jnp.bfloat16),
                kv_ref[i * span : (i + 1) * span, 2 * HD :],
                preferred_element_type=jnp.float32,
            )
        mean = acc / total
        lse = top + jnp.log(total)
        hi = lse.astype(jnp.bfloat16).astype(jnp.float32)
        mid = (lse - hi).astype(jnp.bfloat16).astype(jnp.float32)
        out_ref[pl.ds(at, TILE), 0:VD] = mean[:TILE].astype(jnp.bfloat16)
        out_ref[pl.ds(at, TILE), VD : 2 * VD] = mean[TILE:].astype(jnp.bfloat16)
        out_ref[pl.ds(at, TILE), 2 * VD : 3 * VD] = packed((hi, mid, lse - hi - mid)).astype(
            jnp.bfloat16
        )


def merged(got):
    got = got.astype(jnp.float32)
    means = []
    for m in range(2):
        stat = got[:, :, 2 * VD + 3 * m : 2 * VD + 3 * m + 3]
        lse = stat[..., 0:1] + stat[..., 1:2] + stat[..., 2:3]
        share = jnp.exp(lse - jnp.max(lse, axis=0, keepdims=True))
        acc = jnp.sum(share * got[:, :, m * VD : (m + 1) * VD], axis=0)
        means.append(acc / jnp.sum(share, axis=0))
    return means


def normalize(rows_in, gain):
    values_f = rows_in.astype(jnp.float32)
    scale_inv = lax.rsqrt(jnp.mean(values_f * values_f, axis=-1, keepdims=True) + eps)
    return (values_f * scale_inv * gain).astype(jnp.bfloat16)


def summed_over_tp(shard):
    core = lax.axis_index("c")
    count = lax.axis_size(TP)
    cut = shard.reshape(count // 2, 2, shard.shape[0] // count, shard.shape[1])
    own = jnp.where(core == 0, cut[:, 0], cut[:, 1])
    for_peer = jnp.where(core == 0, cut[:, 1], cut[:, 0])
    from_peer = lax.ppermute(for_peer, "c", [(0, 1), (1, 0)])
    both = (own.astype(jnp.float32) + from_peer.astype(jnp.float32)).astype(jnp.bfloat16)
    tiles = lax.all_to_all(both, "x", 0, 0, tiled=True)
    return jnp.sum(tiles.astype(jnp.float32), axis=0).astype(jnp.bfloat16)


def local(
    residual,
    queries,
    key_pairs,
    values,
    second_weight,
    head_gain,
    out_weight,
    norm_gain,
    up_weight,
    gate_weight,
    conv_weight,
    conv_bias,
    down_weight,
):
    rows = queries.shape[0]
    ff = up_weight.shape[1]
    where = jnp.stack((lax.axis_index("z"), lax.axis_index("y"))).astype(jnp.int32)
    w_rows = up_weight.shape[0]
    width = 2 * ff + ff
    tail = -width % LANES
    cuts = [up_weight, gate_weight, down_weight.T, jnp.zeros((w_rows, tail), jnp.bfloat16)]
    cuts += [queries[i : i + w_rows] for i in range(0, rows, w_rows)]
    row_w = lax.all_gather(jnp.concatenate(cuts, axis=1), "y", axis=0, tiled=True)
    all_w = lax.all_gather(row_w[:, :width], "z", axis=0, tiled=True)
    q_rows = row_w[:, width + tail :]

    kv = jnp.concatenate((key_pairs, values), axis=1)
    last = lax.axis_size("z")
    f5 = shifted(kv, 5, [0, 1, *range(5, last)])
    f11 = shifted(kv, -5, [0, 1, *range(11, last)])
    held = jnp.concatenate((kv, f5, f11), axis=0)
    n1 = shifted(held, 1, range(1, last))
    m1 = shifted(held, -1, [0, *range(4, last)])
    n2 = shifted(n1, 1, range(2, last))
    m2 = shifted(m1, -1, range(3, last))
    e8 = shifted(n2[rows : 2 * rows], 1, range(8, last))
    blocks = [held, n1, m1, n2, m2, e8]
    blocks = [pltpu.with_memory_space_constraint(b, pltpu.VMEM) for b in blocks]
    parts = pl.pallas_call(
        attend_kernel,
        out_shape=jax.ShapeDtypeStruct((NY * rows, 3 * VD), jnp.bfloat16),
        in_specs=[SMEM] + [VMEM] * (1 + len(blocks)),
        out_specs=VMEM,
        scratch_shapes=[
            pltpu.VMEM((NY * rows, 2 * HD), jnp.bfloat16),
            pltpu.VMEM((len(OFFSETS) * rows, 2 * HD + VD), jnp.bfloat16),
        ],
        name="attend",
    )(where, q_rows, *blocks)
    got = lax.all_to_all(parts.reshape(NY, rows, 3 * VD), "y", 0, 0, tiled=True)
    means = merged(got)
    diff = means[0] - second_weight[0] * means[1]
    scale_inv = lax.rsqrt(jnp.mean(diff * diff, axis=-1, keepdims=True) + eps)
    attended = (diff * scale_inv * head_gain * 0.8).astype(jnp.bfloat16)
    proj = summed_over_tp(
        jnp.dot(attended, out_weight, preferred_element_type=jnp.float32).astype(jnp.bfloat16)
    )
    mid = (residual.astype(jnp.float32) + proj.astype(jnp.float32)).astype(jnp.bfloat16)
    normed_all = lax.all_gather(normalize(mid, norm_gain), TP, axis=0, tiled=True)
    count = lax.axis_size("z") * lax.axis_size("y")
    rim_rows = lax.ppermute(normed_all[rows - 8 :], SP, [(i, i + 1) for i in range(count - 1)])
    both = jnp.dot(
        jnp.concatenate((normed_all, rim_rows), axis=0),
        all_w[:, : 2 * ff],
        preferred_element_type=jnp.float32,
    ).astype(jnp.bfloat16)
    up_proj, gate_proj = both[:rows, :ff], both[:rows, ff:]
    taps = conv_weight.shape[0]
    extended = jnp.concatenate((both[rows + 8 - (taps - 1) :, :ff], up_proj), axis=0)
    conv_out = jnp.zeros((rows, ff), jnp.float32) + conv_bias[None, :]
    for tap in range(taps):
        conv_out = conv_out + conv_weight[tap][None, :] * extended[tap : tap + rows].astype(
            jnp.float32
        )
    hidden = (jax.nn.silu(conv_out) * gate_proj.astype(jnp.float32)).astype(jnp.bfloat16)
    ffn = dot_nt(hidden, all_w[:, 2 * ff : width]).astype(jnp.bfloat16)
    ffn_out = summed_over_tp(ffn)
    return (mid.astype(jnp.float32) + ffn_out.astype(jnp.float32)).astype(jnp.bfloat16)


def solution(mesh):
    finer = Mesh(mesh.devices.reshape(NZ, NY, mesh.shape["tp"] // 2, 2), ("z", "y", "x", "c"))
    in_specs = (
        P(SP_TP, None),
        P(SP, TP),
        P(SP, TP),
        P(SP, TP),
        P(TP),
        P(TP),
        P(TP, None),
        P(),
        P(SP, TP),
        P(SP, TP),
        P(None, TP),
        P(TP),
        P(TP, SP),
    )
    out_specs = P(SP_TP, None)
    return jax.shard_map(local, mesh=finer, in_specs=in_specs, out_specs=out_specs, check_vma=False)
```

```python
import jax
import jax.numpy as jnp
from jax import lax
from jax.experimental import pallas as pl
from jax.experimental.pallas import tpu as pltpu
from jax.sharding import Mesh
from jax.sharding import PartitionSpec as P

HD = 64
VD = 128
SP = ("z", "y")
SP_TP = ("z", "y", "x", "c")
TP = ("x", "c")
NZ = 16
NY = 4
eps = 1e-05
neg_fill = -1e30
TILE = 128
LANES = 128
OFFSETS = (0, 5, 11, 1, 6, 12, 15, 4, 10, 2, 7, 13, 14, 3, 9, 8)
CHUNK = 4

VMEM = pl.BlockSpec(memory_space=pltpu.VMEM)
SMEM = pl.BlockSpec(memory_space=pltpu.SMEM)


def shifted(value, steps, targets):
    count = lax.axis_size("z")
    return lax.ppermute(value, "z", [((i - steps) % count, i) for i in targets])


def dot_nt(a, b):
    return lax.dot_general(a, b, (((1,), (1,)), ((), ())), preferred_element_type=jnp.float32)


def row_bias(offsets, rows, z):
    lane = lax.broadcasted_iota(jnp.int32, (1, rows * len(offsets)), 1)
    bias = jnp.zeros(lane.shape, jnp.float32)
    for i, off in enumerate(offsets):
        inside = jnp.logical_and(lane >= i * rows, lane < (i + 1) * rows)
        bias = jnp.where(jnp.logical_and(inside, off > z), neg_fill, bias)
    return bias


def both_maps(q):
    lane = lax.broadcasted_iota(jnp.int32, q.shape, 1)
    q = q * jnp.bfloat16(HD**-0.5)
    zero = jnp.zeros_like(q)
    return jnp.concatenate((jnp.where(lane < HD, q, zero), jnp.where(lane < HD, zero, q)), axis=0)


def packed(columns):
    lane = lax.broadcasted_iota(jnp.int32, (TILE, VD), 1)
    block = jnp.zeros((TILE, VD), jnp.float32)
    for m in range(2):
        for i, v in enumerate(columns):
            column = v[m * TILE : (m + 1) * TILE]
            block = jnp.where(lane == m * len(columns) + i, column, block)
    return block


def attend_kernel(where_ref, rows_ref, *refs):
    blocks, (out_ref, q_ref, kv_ref) = refs[:-3], refs[-3:]
    z = where_ref[0]
    y = where_ref[1]
    rows = kv_ref.shape[0] // len(OFFSETS)
    w_rows = rows_ref.shape[0] // NY
    for i in range(NY * rows // w_rows):
        y_at, lane_at = divmod(i, rows // w_rows)
        q_ref[i * w_rows : (i + 1) * w_rows, :] = rows_ref[
            y_at * w_rows : (y_at + 1) * w_rows, lane_at * 2 * HD : (lane_at + 1) * 2 * HD
        ]
    filled = 0
    for block in blocks:
        kv_ref[filled : filled + block.shape[0], :] = block[...]
        filled += block.shape[0]
    span = CHUNK * rows
    chunks = [OFFSETS[i : i + CHUNK] for i in range(0, len(OFFSETS), CHUNK)]
    biases = [row_bias(offsets, rows, z) for offsets in chunks]

    @pl.loop(0, NY * rows // TILE)
    def _(t):
        at = pl.multiple_of(t * TILE, TILE)
        q2 = both_maps(q_ref[pl.ds(at, TILE), :])
        scores = []
        for i, bias in enumerate(biases):
            keys = kv_ref[i * span : (i + 1) * span, : 2 * HD]
            scores.append(dot_nt(q2, keys) + bias)
        r = lax.broadcasted_iota(jnp.int32, scores[0].shape, 0)
        r = jnp.where(r >= TILE, r - TILE, r) + at
        k = lax.broadcasted_iota(jnp.int32, scores[0].shape, 1)
        hidden = jnp.logical_and(k < rows, k + y * rows > r)
        scores[0] = jnp.where(hidden, neg_fill, scores[0])
        top = jnp.max(scores[0], axis=1, keepdims=True)
        for s in scores[1:]:
            top = jnp.maximum(top, jnp.max(s, axis=1, keepdims=True))
        total = jnp.zeros((2 * TILE, 1), jnp.float32)
        acc = jnp.zeros((2 * TILE, VD), jnp.float32)
        for i, s in enumerate(scores):
            e = jnp.exp(s - top)
            total = total + jnp.sum(e, axis=1, keepdims=True)
            acc = acc + jnp.dot(
                e.astype(jnp.bfloat16),
                kv_ref[i * span : (i + 1) * span, 2 * HD :],
                preferred_element_type=jnp.float32,
            )
        mean = acc / total
        lse = top + jnp.log(total)
        hi = lse.astype(jnp.bfloat16).astype(jnp.float32)
        mid = (lse - hi).astype(jnp.bfloat16).astype(jnp.float32)
        out_ref[pl.ds(at, TILE), 0:VD] = mean[:TILE].astype(jnp.bfloat16)
        out_ref[pl.ds(at, TILE), VD : 2 * VD] = mean[TILE:].astype(jnp.bfloat16)
        out_ref[pl.ds(at, TILE), 2 * VD : 3 * VD] = packed((hi, mid, lse - hi - mid)).astype(
            jnp.bfloat16
        )


def ffn_kernel(rows_ref, rim_ref, w_ref, taps_ref, bias_ref, out_ref, x_ref, acc_ref, held_ref, sems):
    rows, d = rows_ref.shape
    rim = rim_ref.shape[0]
    ff = bias_ref.shape[1]
    pieces = sems.shape[0]
    deep = d // pieces
    copies = []
    for i in range(pieces):
        part = pl.ds(i * deep, deep)
        copies.append(pltpu.make_async_copy(w_ref.at[part, :], held_ref.at[part, :], sems.at[i]))
        copies[-1].start()
    x_ref[:rows, :] = rows_ref[...]
    x_ref[rows:, :] = rim_ref[...]
    for i in range(pieces):
        copies[i].wait()
        part = jnp.dot(
            x_ref[:, i * deep : (i + 1) * deep],
            held_ref[i * deep : (i + 1) * deep, : 2 * ff],
            preferred_element_type=jnp.float32,
        )
        acc_ref[...] = part if i == 0 else acc_ref[...] + part
    up = acc_ref[:, :ff].astype(jnp.bfloat16).astype(jnp.float32)
    gate = acc_ref[:rows, ff : 2 * ff].astype(jnp.bfloat16).astype(jnp.float32)
    before = up[rows:]
    up = up[:rows]
    at = lax.broadcasted_iota(jnp.int32, up.shape, 0)
    one = jnp.where(at == 0, before[rim - 1 : rim], pltpu.roll(up, 1, 0))
    two = pltpu.roll(up, 2, 0)
    two = jnp.where(at == 0, before[rim - 2 : rim - 1], two)
    two = jnp.where(at == 1, before[rim - 1 : rim], two)
    conv = bias_ref[...] + taps_ref[0:1] * two + taps_ref[1:2] * one + taps_ref[2:3] * up
    hidden = (conv / (1.0 + jnp.exp(-conv)) * gate).astype(jnp.bfloat16)
    out_ref[...] = dot_nt(hidden, held_ref[:, 2 * ff :]).astype(jnp.bfloat16)


def merged(got):
    got = got.astype(jnp.float32)
    means = []
    for m in range(2):
        stat = got[:, :, 2 * VD + 3 * m : 2 * VD + 3 * m + 3]
        lse = stat[..., 0:1] + stat[..., 1:2] + stat[..., 2:3]
        share = jnp.exp(lse - jnp.max(lse, axis=0, keepdims=True))
        acc = jnp.sum(share * got[:, :, m * VD : (m + 1) * VD], axis=0)
        means.append(acc / jnp.sum(share, axis=0))
    return means


def normalize(rows_in, gain):
    values_f = rows_in.astype(jnp.float32)
    scale_inv = lax.rsqrt(jnp.mean(values_f * values_f, axis=-1, keepdims=True) + eps)
    return (values_f * scale_inv * gain).astype(jnp.bfloat16)


def summed_over_tp(shard):
    core = lax.axis_index("c")
    count = lax.axis_size(TP)
    cut = shard.reshape(count // 2, 2, shard.shape[0] // count, shard.shape[1])
    own = jnp.where(core == 0, cut[:, 0], cut[:, 1])
    for_peer = jnp.where(core == 0, cut[:, 1], cut[:, 0])
    from_peer = lax.ppermute(for_peer, "c", [(0, 1), (1, 0)])
    both = (own.astype(jnp.float32) + from_peer.astype(jnp.float32)).astype(jnp.bfloat16)
    tiles = lax.all_to_all(both, "x", 0, 0, tiled=True)
    return jnp.sum(tiles.astype(jnp.float32), axis=0).astype(jnp.bfloat16)


def local(
    residual,
    queries,
    key_pairs,
    values,
    second_weight,
    head_gain,
    out_weight,
    norm_gain,
    up_weight,
    gate_weight,
    conv_weight,
    conv_bias,
    down_weight,
):
    rows = queries.shape[0]
    ff = up_weight.shape[1]
    where = jnp.stack((lax.axis_index("z"), lax.axis_index("y"))).astype(jnp.int32)
    w_rows = up_weight.shape[0]
    width = 2 * ff + ff
    tail = -width % LANES
    cuts = [up_weight, gate_weight, down_weight.T, jnp.zeros((w_rows, tail), jnp.bfloat16)]
    cuts += [queries[i : i + w_rows] for i in range(0, rows, w_rows)]
    row_w = lax.all_gather(jnp.concatenate(cuts, axis=1), "y", axis=0, tiled=True)
    all_w = lax.all_gather(row_w[:, :width], "z", axis=0, tiled=True)
    q_rows = row_w[:, width + tail :]

    kv = jnp.concatenate((key_pairs, values), axis=1)
    last = lax.axis_size("z")
    f5 = shifted(kv, 5, [0, 1, *range(5, last)])
    f11 = shifted(kv, -5, [0, 1, *range(11, last)])
    held = jnp.concatenate((kv, f5, f11), axis=0)
    n1 = shifted(held, 1, range(1, last))
    m1 = shifted(held, -1, [0, *range(4, last)])
    n2 = shifted(n1, 1, range(2, last))
    m2 = shifted(m1, -1, range(3, last))
    e8 = shifted(n2[rows : 2 * rows], 1, range(8, last))
    blocks = [held, n1, m1, n2, m2, e8]
    blocks = [pltpu.with_memory_space_constraint(b, pltpu.VMEM) for b in blocks]
    parts = pl.pallas_call(
        attend_kernel,
        out_shape=jax.ShapeDtypeStruct((NY * rows, 3 * VD), jnp.bfloat16),
        in_specs=[SMEM] + [VMEM] * (1 + len(blocks)),
        out_specs=VMEM,
        scratch_shapes=[
            pltpu.VMEM((NY * rows, 2 * HD), jnp.bfloat16),
            pltpu.VMEM((len(OFFSETS) * rows, 2 * HD + VD), jnp.bfloat16),
        ],
        name="attend",
    )(where, q_rows, *blocks)
    got = lax.all_to_all(parts.reshape(NY, rows, 3 * VD), "y", 0, 0, tiled=True)
    means = merged(got)
    diff = means[0] - second_weight[0] * means[1]
    scale_inv = lax.rsqrt(jnp.mean(diff * diff, axis=-1, keepdims=True) + eps)
    attended = (diff * scale_inv * head_gain * 0.8).astype(jnp.bfloat16)
    proj = summed_over_tp(
        jnp.dot(attended, out_weight, preferred_element_type=jnp.float32).astype(jnp.bfloat16)
    )
    mid = (residual.astype(jnp.float32) + proj.astype(jnp.float32)).astype(jnp.bfloat16)
    normed_all = lax.all_gather(normalize(mid, norm_gain), TP, axis=0, tiled=True)
    count = lax.axis_size("z") * lax.axis_size("y")
    rim_rows = lax.ppermute(normed_all[rows - 8 :], SP, [(i, i + 1) for i in range(count - 1)])
    d = normed_all.shape[1]
    in_vmem = [
        pltpu.with_memory_space_constraint(v, pltpu.VMEM) for v in (normed_all, rim_rows)
    ]
    ffn = pl.pallas_call(
        ffn_kernel,
        out_shape=pltpu.VMEM((rows, d), jnp.bfloat16),
        in_specs=[VMEM, VMEM, pl.BlockSpec(memory_space=pl.ANY), VMEM, VMEM],
        out_specs=VMEM,
        scratch_shapes=[
            pltpu.VMEM((rows + rim_rows.shape[0], d), jnp.bfloat16),
            pltpu.VMEM((rows + rim_rows.shape[0], 2 * ff), jnp.float32),
            pltpu.VMEM((d, width), jnp.bfloat16),
            pltpu.SemaphoreType.DMA((8,)),
        ],
        name="ffn",
    )(*in_vmem, all_w, conv_weight, conv_bias.reshape(1, ff))
    ffn_out = summed_over_tp(ffn)
    return (mid.astype(jnp.float32) + ffn_out.astype(jnp.float32)).astype(jnp.bfloat16)


def solution(mesh):
    finer = Mesh(mesh.devices.reshape(NZ, NY, mesh.shape["tp"] // 2, 2), ("z", "y", "x", "c"))
    in_specs = (
        P(SP_TP, None),
        P(SP, TP),
        P(SP, TP),
        P(SP, TP),
        P(TP),
        P(TP),
        P(TP, None),
        P(),
        P(SP, TP),
        P(SP, TP),
        P(None, TP),
        P(TP),
        P(TP, SP),
    )
    out_specs = P(SP_TP, None)
    return jax.shard_map(local, mesh=finer, in_specs=in_specs, out_specs=out_specs, check_vma=False)
```

```python
import jax
import jax.numpy as jnp
from jax import lax
from jax.experimental import pallas as pl
from jax.experimental.pallas import tpu as pltpu
from jax.sharding import Mesh
from jax.sharding import PartitionSpec as P

HD = 64
VD = 128
SP = ("z", "y")
SP_TP = ("z", "y", "x", "c")
TP = ("x", "c")
NZ = 16
NY = 4
eps = 1e-05
neg_fill = -1e30
TILE = 128
LANES = 128
OFFSETS = (0, 5, 11, 1, 6, 12, 15, 4, 10, 2, 7, 13, 14, 3, 9, 8)
CHUNK = 4

VMEM = pl.BlockSpec(memory_space=pltpu.VMEM)
SMEM = pl.BlockSpec(memory_space=pltpu.SMEM)


def shifted(value, steps, targets):
    count = lax.axis_size("z")
    return lax.ppermute(value, "z", [((i - steps) % count, i) for i in targets])


def dot_nt(a, b):
    return lax.dot_general(a, b, (((1,), (1,)), ((), ())), preferred_element_type=jnp.float32)


def row_bias(offsets, rows, z):
    lane = lax.broadcasted_iota(jnp.int32, (1, rows * len(offsets)), 1)
    bias = jnp.zeros(lane.shape, jnp.float32)
    for i, off in enumerate(offsets):
        inside = jnp.logical_and(lane >= i * rows, lane < (i + 1) * rows)
        bias = jnp.where(jnp.logical_and(inside, off > z), neg_fill, bias)
    return bias


def both_maps(q):
    lane = lax.broadcasted_iota(jnp.int32, q.shape, 1)
    q = q * jnp.bfloat16(HD**-0.5)
    zero = jnp.zeros_like(q)
    return jnp.concatenate((jnp.where(lane < HD, q, zero), jnp.where(lane < HD, zero, q)), axis=0)


def packed(columns):
    lane = lax.broadcasted_iota(jnp.int32, (TILE, VD), 1)
    block = jnp.zeros((TILE, VD), jnp.float32)
    for m in range(2):
        for i, v in enumerate(columns):
            column = v[m * TILE : (m + 1) * TILE]
            block = jnp.where(lane == m * len(columns) + i, column, block)
    return block


def attend_kernel(where_ref, rows_ref, *refs):
    blocks, (out_ref, q_ref, kv_ref) = refs[:-3], refs[-3:]
    z = where_ref[0]
    y = where_ref[1]
    rows = kv_ref.shape[0] // len(OFFSETS)
    w_rows = rows_ref.shape[0] // NY
    for i in range(NY * rows // w_rows):
        y_at, lane_at = divmod(i, rows // w_rows)
        q_ref[i * w_rows : (i + 1) * w_rows, :] = rows_ref[
            y_at * w_rows : (y_at + 1) * w_rows, lane_at * 2 * HD : (lane_at + 1) * 2 * HD
        ]
    filled = 0
    for block in blocks:
        kv_ref[filled : filled + block.shape[0], :] = block[...]
        filled += block.shape[0]
    span = CHUNK * rows
    chunks = [OFFSETS[i : i + CHUNK] for i in range(0, len(OFFSETS), CHUNK)]
    biases = [row_bias(offsets, rows, z) for offsets in chunks]

    @pl.loop(0, NY * rows // TILE)
    def _(t):
        at = pl.multiple_of(t * TILE, TILE)
        q2 = both_maps(q_ref[pl.ds(at, TILE), :])
        scores = []
        for i, bias in enumerate(biases):
            keys = kv_ref[i * span : (i + 1) * span, : 2 * HD]
            scores.append(dot_nt(q2, keys) + bias)
        r = lax.broadcasted_iota(jnp.int32, scores[0].shape, 0)
        r = jnp.where(r >= TILE, r - TILE, r) + at
        k = lax.broadcasted_iota(jnp.int32, scores[0].shape, 1)
        hidden = jnp.logical_and(k < rows, k + y * rows > r)
        scores[0] = jnp.where(hidden, neg_fill, scores[0])
        top = jnp.max(scores[0], axis=1, keepdims=True)
        for s in scores[1:]:
            top = jnp.maximum(top, jnp.max(s, axis=1, keepdims=True))
        total = jnp.zeros((2 * TILE, 1), jnp.float32)
        acc = jnp.zeros((2 * TILE, VD), jnp.float32)
        for i, s in enumerate(scores):
            e = jnp.exp(s - top)
            total = total + jnp.sum(e, axis=1, keepdims=True)
            acc = acc + jnp.dot(
                e.astype(jnp.bfloat16),
                kv_ref[i * span : (i + 1) * span, 2 * HD :],
                preferred_element_type=jnp.float32,
            )
        mean = acc / total
        lse = top + jnp.log(total)
        hi = lse.astype(jnp.bfloat16).astype(jnp.float32)
        mid = (lse - hi).astype(jnp.bfloat16).astype(jnp.float32)
        out_ref[pl.ds(at, TILE), 0:VD] = mean[:TILE].astype(jnp.bfloat16)
        out_ref[pl.ds(at, TILE), VD : 2 * VD] = mean[TILE:].astype(jnp.bfloat16)
        out_ref[pl.ds(at, TILE), 2 * VD : 3 * VD] = packed((hi, mid, lse - hi - mid)).astype(
            jnp.bfloat16
        )


def ffn_kernel(rows_ref, rim_ref, w_ref, taps_ref, bias_ref, out_ref, x_ref, acc_ref, held_ref, sems):
    rows = rows_ref.shape[0]
    rim = rim_ref.shape[0]
    ff = bias_ref.shape[1]
    edges = [*range(0, 2 * ff - 2 * LANES, 4 * LANES), 2 * ff, 3 * ff]
    copies = []
    for i, (start, end) in enumerate(zip(edges, edges[1:])):
        part = pl.ds(start, end - start)
        copies.append(pltpu.make_async_copy(w_ref.at[:, part], held_ref.at[:, part], sems.at[i]))
        copies[-1].start()
    x_ref[:rows, :] = rows_ref[...]
    x_ref[rows:, :] = rim_ref[...]
    for i, (start, end) in enumerate(zip(edges[:-1], edges[1:-1])):
        copies[i].wait()
        acc_ref[:, start:end] = jnp.dot(
            x_ref[...], held_ref[:, start:end], preferred_element_type=jnp.float32
        ).astype(jnp.bfloat16)
    up = acc_ref[:, :ff].astype(jnp.float32)
    gate = acc_ref[:rows, ff : 2 * ff].astype(jnp.float32)
    before = up[rows:]
    up = up[:rows]
    at = lax.broadcasted_iota(jnp.int32, up.shape, 0)
    one = jnp.where(at == 0, before[rim - 1 : rim], pltpu.roll(up, 1, 0))
    two = pltpu.roll(up, 2, 0)
    two = jnp.where(at == 0, before[rim - 2 : rim - 1], two)
    two = jnp.where(at == 1, before[rim - 1 : rim], two)
    conv = bias_ref[...] + taps_ref[0:1] * two + taps_ref[1:2] * one + taps_ref[2:3] * up
    hidden = (conv / (1.0 + jnp.exp(-conv)) * gate).astype(jnp.bfloat16)
    copies[-1].wait()
    out_ref[...] = dot_nt(hidden, held_ref[:, 2 * ff :]).astype(jnp.bfloat16)


def merged(got):
    got = got.astype(jnp.float32)
    means = []
    for m in range(2):
        stat = got[:, :, 2 * VD + 3 * m : 2 * VD + 3 * m + 3]
        lse = stat[..., 0:1] + stat[..., 1:2] + stat[..., 2:3]
        share = jnp.exp(lse - jnp.max(lse, axis=0, keepdims=True))
        acc = jnp.sum(share * got[:, :, m * VD : (m + 1) * VD], axis=0)
        means.append(acc / jnp.sum(share, axis=0))
    return means


def normalize(rows_in, gain):
    values_f = rows_in.astype(jnp.float32)
    scale_inv = lax.rsqrt(jnp.mean(values_f * values_f, axis=-1, keepdims=True) + eps)
    return (values_f * scale_inv * gain).astype(jnp.bfloat16)


def summed_over_tp(shard):
    core = lax.axis_index("c")
    count = lax.axis_size(TP)
    cut = shard.reshape(count // 2, 2, shard.shape[0] // count, shard.shape[1])
    own = jnp.where(core == 0, cut[:, 0], cut[:, 1])
    for_peer = jnp.where(core == 0, cut[:, 1], cut[:, 0])
    from_peer = lax.ppermute(for_peer, "c", [(0, 1), (1, 0)])
    both = (own.astype(jnp.float32) + from_peer.astype(jnp.float32)).astype(jnp.bfloat16)
    tiles = lax.all_to_all(both, "x", 0, 0, tiled=True)
    return jnp.sum(tiles.astype(jnp.float32), axis=0).astype(jnp.bfloat16)


def local(
    residual,
    queries,
    key_pairs,
    values,
    second_weight,
    head_gain,
    out_weight,
    norm_gain,
    up_weight,
    gate_weight,
    conv_weight,
    conv_bias,
    down_weight,
):
    rows = queries.shape[0]
    ff = up_weight.shape[1]
    where = jnp.stack((lax.axis_index("z"), lax.axis_index("y"))).astype(jnp.int32)
    w_rows = up_weight.shape[0]
    width = 2 * ff + ff
    tail = -width % LANES
    cuts = [up_weight, gate_weight, down_weight.T, jnp.zeros((w_rows, tail), jnp.bfloat16)]
    cuts += [queries[i : i + w_rows] for i in range(0, rows, w_rows)]
    row_w = lax.all_gather(jnp.concatenate(cuts, axis=1), "y", axis=0, tiled=True)
    all_w = lax.all_gather(row_w[:, :width], "z", axis=0, tiled=True)
    q_rows = row_w[:, width + tail :]

    kv = jnp.concatenate((key_pairs, values), axis=1)
    last = lax.axis_size("z")
    f5 = shifted(kv, 5, [0, 1, *range(5, last)])
    f11 = shifted(kv, -5, [0, 1, *range(11, last)])
    held = jnp.concatenate((kv, f5, f11), axis=0)
    n1 = shifted(held, 1, range(1, last))
    m1 = shifted(held, -1, [0, *range(4, last)])
    n2 = shifted(n1, 1, range(2, last))
    m2 = shifted(m1, -1, range(3, last))
    e8 = shifted(n2[rows : 2 * rows], 1, range(8, last))
    blocks = [held, n1, m1, n2, m2, e8]
    blocks = [pltpu.with_memory_space_constraint(b, pltpu.VMEM) for b in blocks]
    parts = pl.pallas_call(
        attend_kernel,
        out_shape=pltpu.VMEM((NY * rows, 3 * VD), jnp.bfloat16),
        in_specs=[SMEM] + [VMEM] * (1 + len(blocks)),
        out_specs=VMEM,
        scratch_shapes=[
            pltpu.VMEM((NY * rows, 2 * HD), jnp.bfloat16),
            pltpu.VMEM((len(OFFSETS) * rows, 2 * HD + VD), jnp.bfloat16),
        ],
        name="attend",
    )(where, q_rows, *blocks)
    got = lax.all_to_all(parts.reshape(NY, rows, 3 * VD), "y", 0, 0, tiled=True)
    means = merged(got)
    diff = means[0] - second_weight[0] * means[1]
    scale_inv = lax.rsqrt(jnp.mean(diff * diff, axis=-1, keepdims=True) + eps)
    attended = (diff * scale_inv * head_gain * 0.8).astype(jnp.bfloat16)
    proj = summed_over_tp(
        jnp.dot(attended, out_weight, preferred_element_type=jnp.float32).astype(jnp.bfloat16)
    )
    mid = (residual.astype(jnp.float32) + proj.astype(jnp.float32)).astype(jnp.bfloat16)
    normed_all = lax.all_gather(normalize(mid, norm_gain), TP, axis=0, tiled=True)
    count = lax.axis_size("z") * lax.axis_size("y")
    rim_rows = lax.ppermute(normed_all[rows - 8 :], SP, [(i, i + 1) for i in range(count - 1)])
    d = normed_all.shape[1]
    in_vmem = [
        pltpu.with_memory_space_constraint(v, pltpu.VMEM) for v in (normed_all, rim_rows)
    ]
    ffn = pl.pallas_call(
        ffn_kernel,
        out_shape=pltpu.VMEM((rows, d), jnp.bfloat16),
        in_specs=[VMEM, VMEM, pl.BlockSpec(memory_space=pl.ANY), VMEM, VMEM],
        out_specs=VMEM,
        scratch_shapes=[
            pltpu.VMEM((rows + rim_rows.shape[0], d), jnp.bfloat16),
            pltpu.VMEM((rows + rim_rows.shape[0], 2 * ff), jnp.bfloat16),
            pltpu.VMEM((d, width), jnp.bfloat16),
            pltpu.SemaphoreType.DMA((4,)),
        ],
        name="ffn",
    )(*in_vmem, all_w, conv_weight, conv_bias.reshape(1, ff))
    ffn_out = summed_over_tp(ffn)
    return (mid.astype(jnp.float32) + ffn_out.astype(jnp.float32)).astype(jnp.bfloat16)


def solution(mesh):
    finer = Mesh(mesh.devices.reshape(NZ, NY, mesh.shape["tp"] // 2, 2), ("z", "y", "x", "c"))
    in_specs = (
        P(SP_TP, None),
        P(SP, TP),
        P(SP, TP),
        P(SP, TP),
        P(TP),
        P(TP),
        P(TP, None),
        P(),
        P(SP, TP),
        P(SP, TP),
        P(None, TP),
        P(TP),
        P(TP, SP),
    )
    out_specs = P(SP_TP, None)
    return jax.shard_map(local, mesh=finer, in_specs=in_specs, out_specs=out_specs, check_vma=False)
```

```python
import jax
import jax.numpy as jnp
from jax import lax
from jax.experimental import pallas as pl
from jax.experimental.pallas import tpu as pltpu
from jax.sharding import Mesh
from jax.sharding import PartitionSpec as P

HD = 64
VD = 128
SP = ("z", "y")
SP_TP = ("z", "y", "x", "c")
TP = ("x", "c")
NZ = 16
NY = 4
eps = 1e-05
neg_fill = -1e30
TILE = 384
LANES = 128
OFFSETS = (0, 5, 11, 1, 6, 12, 15, 4, 10, 2, 7, 13, 14, 3, 9, 8)
CHUNK = 4

VMEM = pl.BlockSpec(memory_space=pltpu.VMEM)
SMEM = pl.BlockSpec(memory_space=pltpu.SMEM)


def shifted(value, steps, targets):
    count = lax.axis_size("z")
    return lax.ppermute(value, "z", [((i - steps) % count, i) for i in targets])


def dot_nt(a, b):
    return lax.dot_general(a, b, (((1,), (1,)), ((), ())), preferred_element_type=jnp.float32)


def row_bias(offsets, rows, z):
    lane = lax.broadcasted_iota(jnp.int32, (1, rows * len(offsets)), 1)
    bias = jnp.zeros(lane.shape, jnp.float32)
    for i, off in enumerate(offsets):
        inside = jnp.logical_and(lane >= i * rows, lane < (i + 1) * rows)
        bias = jnp.where(jnp.logical_and(inside, off > z), neg_fill, bias)
    return bias


def both_maps(q):
    lane = lax.broadcasted_iota(jnp.int32, q.shape, 1)
    q = q * jnp.bfloat16(HD**-0.5)
    zero = jnp.zeros_like(q)
    return jnp.concatenate((jnp.where(lane < HD, q, zero), jnp.where(lane < HD, zero, q)), axis=0)


def packed(columns):
    lane = lax.broadcasted_iota(jnp.int32, (TILE, VD), 1)
    block = jnp.zeros((TILE, VD), jnp.float32)
    for m in range(2):
        for i, v in enumerate(columns):
            column = v[m * TILE : (m + 1) * TILE]
            block = jnp.where(lane == m * len(columns) + i, column, block)
    return block


def attend_kernel(where_ref, rows_ref, *refs):
    blocks, (out_ref, q_ref, kv_ref) = refs[:-3], refs[-3:]
    z = where_ref[0]
    y = where_ref[1]
    rows = kv_ref.shape[0] // len(OFFSETS)
    w_rows = rows_ref.shape[0] // NY
    for i in range(NY * rows // w_rows):
        y_at, lane_at = divmod(i, rows // w_rows)
        q_ref[i * w_rows : (i + 1) * w_rows, :] = rows_ref[
            y_at * w_rows : (y_at + 1) * w_rows, lane_at * 2 * HD : (lane_at + 1) * 2 * HD
        ]
    filled = 0
    for block in blocks:
        kv_ref[filled : filled + block.shape[0], :] = block[...]
        filled += block.shape[0]
    span = CHUNK * rows
    chunks = [OFFSETS[i : i + CHUNK] for i in range(0, len(OFFSETS), CHUNK)]
    biases = [row_bias(offsets, rows, z) for offsets in chunks]

    @pl.loop(0, NY * rows // TILE)
    def _(t):
        at = pl.multiple_of(t * TILE, TILE)
        q2 = both_maps(q_ref[pl.ds(at, TILE), :])
        scores = []
        for i, bias in enumerate(biases):
            keys = kv_ref[i * span : (i + 1) * span, : 2 * HD]
            scores.append(dot_nt(q2, keys) + bias)
        r = lax.broadcasted_iota(jnp.int32, scores[0].shape, 0)
        r = jnp.where(r >= TILE, r - TILE, r) + at
        k = lax.broadcasted_iota(jnp.int32, scores[0].shape, 1)
        hidden = jnp.logical_and(k < rows, k + y * rows > r)
        scores[0] = jnp.where(hidden, neg_fill, scores[0])
        top = jnp.max(scores[0], axis=1, keepdims=True)
        for s in scores[1:]:
            top = jnp.maximum(top, jnp.max(s, axis=1, keepdims=True))
        total = jnp.zeros((2 * TILE, 1), jnp.float32)
        acc = jnp.zeros((2 * TILE, VD), jnp.float32)
        for i, s in enumerate(scores):
            e = jnp.exp(s - top)
            total = total + jnp.sum(e, axis=1, keepdims=True)
            acc = acc + jnp.dot(
                e.astype(jnp.bfloat16),
                kv_ref[i * span : (i + 1) * span, 2 * HD :],
                preferred_element_type=jnp.float32,
            )
        mean = acc / total
        lse = top + jnp.log(total)
        hi = lse.astype(jnp.bfloat16).astype(jnp.float32)
        mid = (lse - hi).astype(jnp.bfloat16).astype(jnp.float32)
        out_ref[pl.ds(at, TILE), 0:VD] = mean[:TILE].astype(jnp.bfloat16)
        out_ref[pl.ds(at, TILE), VD : 2 * VD] = mean[TILE:].astype(jnp.bfloat16)
        out_ref[pl.ds(at, TILE), 2 * VD : 3 * VD] = packed((hi, mid, lse - hi - mid)).astype(
            jnp.bfloat16
        )


def fold_kernel(rows_ref, out_ref, q_ref):
    deep = rows_ref.shape[0]
    blocks = out_ref.shape[0] // deep
    for i in range(blocks):
        out_ref[i * deep : (i + 1) * deep, :] = rows_ref[:, i * LANES : (i + 1) * LANES]
    last = rows_ref[:, blocks * LANES : (blocks + 1) * LANES].astype(jnp.float32)
    lane = lax.broadcasted_iota(jnp.int32, (deep // 2, LANES), 1)
    low, high = last[: deep // 2], pltpu.roll(last[deep // 2 :], LANES // 2, 1)
    out_ref[blocks * deep :, :] = jnp.where(lane < LANES // 2, low, high).astype(jnp.bfloat16)
    q_ref[...] = rows_ref[:, (blocks + 1) * LANES :]


def ffn_kernel(
    rows_ref, rim_ref, w_ref, taps_ref, bias_ref, out_ref, x_ref, acc_ref, held_ref, tail_ref, sems
):
    rows, d = rows_ref.shape
    rim = rim_ref.shape[0]
    ff = bias_ref.shape[1]
    count, deep, _ = held_ref.shape
    full = 3 * ff // LANES
    copies = []
    for i in range(full):
        copies.append(
            pltpu.make_async_copy(
                w_ref.at[:, pl.ds(i * deep, deep), :],
                held_ref.at[:, :, pl.ds(i * LANES, LANES)],
                sems.at[i],
            )
        )
        copies[-1].start()
    copies.append(
        pltpu.make_async_copy(
            w_ref.at[:, pl.ds(full * deep, deep // 2), :], tail_ref, sems.at[full]
        )
    )
    copies[-1].start()
    edges = [*range(0, 2 * ff - 2 * LANES, 4 * LANES), 2 * ff]
    x_ref[:rows, :] = rows_ref[...]
    x_ref[rows:, :] = rim_ref[...]
    for start, end in zip(edges, edges[1:]):
        for i in range(start // LANES, end // LANES):
            copies[i].wait()
        acc_ref[:, start:end] = jnp.dot(
            x_ref[...],
            held_ref[:, :, start:end].reshape(d, end - start),
            preferred_element_type=jnp.float32,
        ).astype(jnp.bfloat16)
    up = acc_ref[:, :ff].astype(jnp.float32)
    gate = acc_ref[:rows, ff : 2 * ff].astype(jnp.float32)
    before = up[rows:]
    up = up[:rows]
    at = lax.broadcasted_iota(jnp.int32, up.shape, 0)
    one = jnp.where(at == 0, before[rim - 1 : rim], pltpu.roll(up, 1, 0))
    two = pltpu.roll(up, 2, 0)
    two = jnp.where(at == 0, before[rim - 2 : rim - 1], two)
    two = jnp.where(at == 1, before[rim - 1 : rim], two)
    conv = bias_ref[...] + taps_ref[0:1] * two + taps_ref[1:2] * one + taps_ref[2:3] * up
    hidden = (conv / (1.0 + jnp.exp(-conv)) * gate).astype(jnp.bfloat16)
    for copy in copies[2 * ff // LANES :]:
        copy.wait()
    tail = tail_ref[...].reshape(count * deep // 2, LANES).astype(jnp.float32)
    pair = (tail, pltpu.roll(tail, LANES // 2, 1))
    for i, half in enumerate(pair):
        block = half.astype(jnp.bfloat16).reshape(count, deep // 2, LANES)
        held_ref[:, i * deep // 2 : (i + 1) * deep // 2, full * LANES :] = block
    down = held_ref[:, :, 2 * ff : 3 * ff].reshape(d, ff)
    out_ref[...] = dot_nt(hidden, down).astype(jnp.bfloat16)


def merged(got):
    got = got.astype(jnp.float32)
    means = []
    for m in range(2):
        stat = got[:, :, 2 * VD + 3 * m : 2 * VD + 3 * m + 3]
        lse = stat[..., 0:1] + stat[..., 1:2] + stat[..., 2:3]
        share = jnp.exp(lse - jnp.max(lse, axis=0, keepdims=True))
        acc = jnp.sum(share * got[:, :, m * VD : (m + 1) * VD], axis=0)
        means.append(acc / jnp.sum(share, axis=0))
    return means


def normalize(rows_in, gain):
    values_f = rows_in.astype(jnp.float32)
    scale_inv = lax.rsqrt(jnp.mean(values_f * values_f, axis=-1, keepdims=True) + eps)
    return (values_f * scale_inv * gain).astype(jnp.bfloat16)


def summed_over_tp(shard):
    core = lax.axis_index("c")
    count = lax.axis_size(TP)
    cut = shard.reshape(count // 2, 2, shard.shape[0] // count, shard.shape[1])
    own = jnp.where(core == 0, cut[:, 0], cut[:, 1])
    for_peer = jnp.where(core == 0, cut[:, 1], cut[:, 0])
    from_peer = lax.ppermute(for_peer, "c", [(0, 1), (1, 0)])
    both = (own.astype(jnp.float32) + from_peer.astype(jnp.float32)).astype(jnp.bfloat16)
    tiles = lax.all_to_all(both, "x", 0, 0, tiled=True)
    return jnp.sum(tiles.astype(jnp.float32), axis=0).astype(jnp.bfloat16)


def local(
    residual,
    queries,
    key_pairs,
    values,
    second_weight,
    head_gain,
    out_weight,
    norm_gain,
    up_weight,
    gate_weight,
    conv_weight,
    conv_bias,
    down_weight,
):
    rows = queries.shape[0]
    ff = up_weight.shape[1]
    where = jnp.stack((lax.axis_index("z"), lax.axis_index("y"))).astype(jnp.int32)
    w_rows = up_weight.shape[0]
    width = 2 * ff + ff
    tail = -width % LANES
    cuts = [up_weight, gate_weight, down_weight.T, jnp.zeros((w_rows, tail), jnp.bfloat16)]
    cuts += [queries[i : i + w_rows] for i in range(0, rows, w_rows)]
    row_w = lax.all_gather(jnp.concatenate(cuts, axis=1), "y", axis=0, tiled=True)
    deep = row_w.shape[0]
    shard, q_rows = pl.pallas_call(
        fold_kernel,
        out_shape=[
            jax.ShapeDtypeStruct((deep * width // LANES, LANES), jnp.bfloat16),
            pltpu.VMEM((deep, row_w.shape[1] - width - tail), jnp.bfloat16),
        ],
        in_specs=[VMEM],
        out_specs=[VMEM] * 2,
        name="fold",
    )(pltpu.with_memory_space_constraint(row_w, pltpu.VMEM))
    all_w = lax.all_gather(shard, "z", axis=0, tiled=True)
    all_w = all_w.reshape(-1, *shard.shape)

    kv = jnp.concatenate((key_pairs, values), axis=1)
    last = lax.axis_size("z")
    f5 = shifted(kv, 5, [0, 1, *range(5, last)])
    f11 = shifted(kv, -5, [0, 1, *range(11, last)])
    held = jnp.concatenate((kv, f5, f11), axis=0)
    n1 = shifted(held, 1, range(1, last))
    m1 = shifted(held, -1, [0, *range(4, last)])
    n2 = shifted(n1, 1, range(2, last))
    m2 = shifted(m1, -1, range(3, last))
    e8 = shifted(n2[rows : 2 * rows], 1, range(8, last))
    blocks = [held, n1, m1, n2, m2, e8]
    blocks = [pltpu.with_memory_space_constraint(b, pltpu.VMEM) for b in blocks]
    parts = pl.pallas_call(
        attend_kernel,
        out_shape=pltpu.VMEM((NY * rows, 3 * VD), jnp.bfloat16),
        in_specs=[SMEM] + [VMEM] * (1 + len(blocks)),
        out_specs=VMEM,
        scratch_shapes=[
            pltpu.VMEM((NY * rows, 2 * HD), jnp.bfloat16),
            pltpu.VMEM((len(OFFSETS) * rows, 2 * HD + VD), jnp.bfloat16),
        ],
        name="attend",
    )(where, q_rows, *blocks)
    got = lax.all_to_all(parts.reshape(NY, rows, 3 * VD), "y", 0, 0, tiled=True)
    means = merged(got)
    diff = means[0] - second_weight[0] * means[1]
    scale_inv = lax.rsqrt(jnp.mean(diff * diff, axis=-1, keepdims=True) + eps)
    attended = (diff * scale_inv * head_gain * 0.8).astype(jnp.bfloat16)
    proj = summed_over_tp(
        jnp.dot(attended, out_weight, preferred_element_type=jnp.float32).astype(jnp.bfloat16)
    )
    mid = (residual.astype(jnp.float32) + proj.astype(jnp.float32)).astype(jnp.bfloat16)
    normed_all = lax.all_gather(normalize(mid, norm_gain), TP, axis=0, tiled=True)
    count = lax.axis_size("z") * lax.axis_size("y")
    rim_rows = lax.ppermute(normed_all[rows - 8 :], SP, [(i, i + 1) for i in range(count - 1)])
    d = normed_all.shape[1]
    in_vmem = [
        pltpu.with_memory_space_constraint(v, pltpu.VMEM) for v in (normed_all, rim_rows)
    ]
    ffn = pl.pallas_call(
        ffn_kernel,
        out_shape=pltpu.VMEM((rows, d), jnp.bfloat16),
        in_specs=[VMEM, VMEM, pl.BlockSpec(memory_space=pl.ANY), VMEM, VMEM],
        out_specs=VMEM,
        scratch_shapes=[
            pltpu.VMEM((rows + rim_rows.shape[0], d), jnp.bfloat16),
            pltpu.VMEM((rows + rim_rows.shape[0], 2 * ff), jnp.bfloat16),
            pltpu.VMEM((all_w.shape[0], deep, width + tail), jnp.bfloat16),
            pltpu.VMEM((all_w.shape[0], deep // 2, LANES), jnp.bfloat16),
            pltpu.SemaphoreType.DMA((width // LANES + 1,)),
        ],
        name="ffn",
    )(*in_vmem, all_w, conv_weight, conv_bias.reshape(1, ff))
    ffn_out = summed_over_tp(ffn)
    return (mid.astype(jnp.float32) + ffn_out.astype(jnp.float32)).astype(jnp.bfloat16)


def solution(mesh):
    finer = Mesh(mesh.devices.reshape(NZ, NY, mesh.shape["tp"] // 2, 2), ("z", "y", "x", "c"))
    in_specs = (
        P(SP_TP, None),
        P(SP, TP),
        P(SP, TP),
        P(SP, TP),
        P(TP),
        P(TP),
        P(TP, None),
        P(),
        P(SP, TP),
        P(SP, TP),
        P(None, TP),
        P(TP),
        P(TP, SP),
    )
    out_specs = P(SP_TP, None)
    return jax.shard_map(local, mesh=finer, in_specs=in_specs, out_specs=out_specs, check_vma=False)
```

```python
import jax
import jax.numpy as jnp
from jax import lax
from jax.experimental import pallas as pl
from jax.experimental.pallas import tpu as pltpu
from jax.sharding import Mesh
from jax.sharding import PartitionSpec as P

HD = 64
VD = 128
SP = ("z", "y")
SP_TP = ("z", "y", "x", "c")
TP = ("x", "c")
NZ = 16
NY = 4
eps = 1e-05
neg_fill = -1e30
TILE = 128
LANES = 128
OFFSETS = (0, 5, 11, 1, 6, 12, 15, 4, 10, 2, 7, 13, 14, 3, 9, 8)
CHUNK = 2

VMEM = pl.BlockSpec(memory_space=pltpu.VMEM)
SMEM = pl.BlockSpec(memory_space=pltpu.SMEM)


def shifted(value, steps, targets):
    count = lax.axis_size("z")
    return lax.ppermute(value, "z", [((i - steps) % count, i) for i in targets])


def dot_nt(a, b):
    return lax.dot_general(a, b, (((1,), (1,)), ((), ())), preferred_element_type=jnp.float32)


def row_bias(offsets, rows, z):
    lane = lax.broadcasted_iota(jnp.int32, (1, rows * len(offsets)), 1)
    bias = jnp.zeros(lane.shape, jnp.float32)
    for i, off in enumerate(offsets):
        inside = jnp.logical_and(lane >= i * rows, lane < (i + 1) * rows)
        bias = jnp.where(jnp.logical_and(inside, off > z), neg_fill, bias)
    return bias


def both_maps(q):
    lane = lax.broadcasted_iota(jnp.int32, q.shape, 1)
    q = q * jnp.bfloat16(HD**-0.5)
    zero = jnp.zeros_like(q)
    return jnp.concatenate((jnp.where(lane < HD, q, zero), jnp.where(lane < HD, zero, q)), axis=0)


def packed(columns):
    lane = lax.broadcasted_iota(jnp.int32, (TILE, VD), 1)
    block = jnp.zeros((TILE, VD), jnp.float32)
    for m in range(2):
        for i, v in enumerate(columns):
            column = v[m * TILE : (m + 1) * TILE]
            block = jnp.where(lane == m * len(columns) + i, column, block)
    return block


def attend_kernel(where_ref, rows_ref, *refs):
    blocks, (out_ref, q_ref, kv_ref) = refs[:-3], refs[-3:]
    z = where_ref[0]
    y = where_ref[1]
    rows = kv_ref.shape[0] // len(OFFSETS)
    w_rows = rows_ref.shape[0] // NY
    for i in range(NY * rows // w_rows):
        y_at, lane_at = divmod(i, rows // w_rows)
        q_ref[i * w_rows : (i + 1) * w_rows, :] = rows_ref[
            y_at * w_rows : (y_at + 1) * w_rows, lane_at * 2 * HD : (lane_at + 1) * 2 * HD
        ]
    filled = 0
    for block in blocks:
        kv_ref[filled : filled + block.shape[0], :] = block[...]
        filled += block.shape[0]
    span = CHUNK * rows
    chunks = [OFFSETS[i : i + CHUNK] for i in range(0, len(OFFSETS), CHUNK)]
    biases = [row_bias(offsets, rows, z) for offsets in chunks]

    @pl.loop(0, NY * rows // TILE)
    def _(t):
        at = pl.multiple_of(t * TILE, TILE)
        q2 = both_maps(q_ref[pl.ds(at, TILE), :])
        scores = []
        for i, bias in enumerate(biases):
            keys = kv_ref[i * span : (i + 1) * span, : 2 * HD]
            scores.append(dot_nt(q2, keys) + bias)
        r = lax.broadcasted_iota(jnp.int32, scores[0].shape, 0)
        r = jnp.where(r >= TILE, r - TILE, r) + at
        k = lax.broadcasted_iota(jnp.int32, scores[0].shape, 1)
        hidden = jnp.logical_and(k < rows, k + y * rows > r)
        scores[0] = jnp.where(hidden, neg_fill, scores[0])
        top = jnp.max(scores[0], axis=1, keepdims=True)
        for s in scores[1:]:
            top = jnp.maximum(top, jnp.max(s, axis=1, keepdims=True))
        total = jnp.zeros((2 * TILE, 1), jnp.float32)
        acc = jnp.zeros((2 * TILE, VD), jnp.float32)
        for i, s in enumerate(scores):
            e = jnp.exp(s - top)
            total = total + jnp.sum(e, axis=1, keepdims=True)
            acc = acc + jnp.dot(
                e.astype(jnp.bfloat16),
                kv_ref[i * span : (i + 1) * span, 2 * HD :],
                preferred_element_type=jnp.float32,
            )
        mean = acc / total
        lse = top + jnp.log(total)
        hi = lse.astype(jnp.bfloat16).astype(jnp.float32)
        mid = (lse - hi).astype(jnp.bfloat16).astype(jnp.float32)
        out_ref[pl.ds(at, TILE), 0:VD] = mean[:TILE].astype(jnp.bfloat16)
        out_ref[pl.ds(at, TILE), VD : 2 * VD] = mean[TILE:].astype(jnp.bfloat16)
        out_ref[pl.ds(at, TILE), 2 * VD : 3 * VD] = packed((hi, mid, lse - hi - mid)).astype(
            jnp.bfloat16
        )


def fold_kernel(rows_ref, out_ref, q_ref):
    deep = rows_ref.shape[0]
    blocks = out_ref.shape[0] // deep
    for i in range(blocks):
        out_ref[i * deep : (i + 1) * deep, :] = rows_ref[:, i * LANES : (i + 1) * LANES]
    last = rows_ref[:, blocks * LANES : (blocks + 1) * LANES].astype(jnp.float32)
    lane = lax.broadcasted_iota(jnp.int32, (deep // 2, LANES), 1)
    low, high = last[: deep // 2], pltpu.roll(last[deep // 2 :], LANES // 2, 1)
    out_ref[blocks * deep :, :] = jnp.where(lane < LANES // 2, low, high).astype(jnp.bfloat16)
    q_ref[...] = rows_ref[:, (blocks + 1) * LANES :]


def ffn_kernel(
    rows_ref, rim_ref, w_ref, taps_ref, bias_ref, out_ref, x_ref, acc_ref, held_ref, tail_ref, sems
):
    rows, d = rows_ref.shape
    rim = rim_ref.shape[0]
    ff = bias_ref.shape[0]
    count, deep, _ = held_ref.shape
    full = 3 * ff // LANES
    copies = []
    for i in range(full):
        copies.append(
            pltpu.make_async_copy(
                w_ref.at[:, pl.ds(i * deep, deep), :],
                held_ref.at[:, :, pl.ds(i * LANES, LANES)],
                sems.at[i],
            )
        )
        copies[-1].start()
    copies.append(
        pltpu.make_async_copy(
            w_ref.at[:, pl.ds(full * deep, deep // 2), :], tail_ref, sems.at[full]
        )
    )
    copies[-1].start()
    edges = [*range(0, 2 * ff - 2 * LANES, 4 * LANES), 2 * ff]
    x_ref[:rows, :] = rows_ref[...]
    x_ref[rows:, :] = rim_ref[...]
    for start, end in zip(edges, edges[1:]):
        for i in range(start // LANES, end // LANES):
            copies[i].wait()
        acc_ref[:, start:end] = jnp.dot(
            x_ref[...],
            held_ref[:, :, start:end].reshape(d, end - start),
            preferred_element_type=jnp.float32,
        ).astype(jnp.bfloat16)
    up = acc_ref[:, :ff].astype(jnp.float32)
    gate = acc_ref[:rows, ff : 2 * ff].astype(jnp.float32)
    before = up[rows:]
    up = up[:rows]
    at = lax.broadcasted_iota(jnp.int32, up.shape, 0)
    one = jnp.where(at == 0, before[rim - 1 : rim], pltpu.roll(up, 1, 0))
    two = pltpu.roll(up, 2, 0)
    two = jnp.where(at == 0, before[rim - 2 : rim - 1], two)
    two = jnp.where(at == 1, before[rim - 1 : rim], two)
    conv = bias_ref[...].reshape(1, ff) + taps_ref[0:1] * two + taps_ref[1:2] * one + taps_ref[2:3] * up
    hidden = (conv / (1.0 + jnp.exp(-conv)) * gate).astype(jnp.bfloat16)
    for copy in copies[2 * ff // LANES :]:
        copy.wait()
    tail = tail_ref[...].reshape(count * deep // 2, LANES).astype(jnp.float32)
    pair = (tail, pltpu.roll(tail, LANES // 2, 1))
    for i, half in enumerate(pair):
        block = half.astype(jnp.bfloat16).reshape(count, deep // 2, LANES)
        held_ref[:, i * deep // 2 : (i + 1) * deep // 2, full * LANES :] = block
    down = held_ref[:, :, 2 * ff : 3 * ff].reshape(d, ff)
    out_ref[...] = dot_nt(hidden, down).astype(jnp.bfloat16)


def merged(got):
    got = got.astype(jnp.float32)
    means = []
    for m in range(2):
        stat = got[:, :, 2 * VD + 3 * m : 2 * VD + 3 * m + 3]
        lse = stat[..., 0:1] + stat[..., 1:2] + stat[..., 2:3]
        share = jnp.exp(lse - jnp.max(lse, axis=0, keepdims=True))
        acc = jnp.sum(share * got[:, :, m * VD : (m + 1) * VD], axis=0)
        means.append(acc / jnp.sum(share, axis=0))
    return means


def normalize(rows_in, gain):
    values_f = rows_in.astype(jnp.float32)
    scale_inv = lax.rsqrt(jnp.mean(values_f * values_f, axis=-1, keepdims=True) + eps)
    return (values_f * scale_inv * gain).astype(jnp.bfloat16)


def summed_over_tp(shard):
    core = lax.axis_index("c")
    count = lax.axis_size(TP)
    cut = shard.reshape(count // 2, 2, shard.shape[0] // count, shard.shape[1])
    own = jnp.where(core == 0, cut[:, 0], cut[:, 1])
    for_peer = jnp.where(core == 0, cut[:, 1], cut[:, 0])
    from_peer = lax.ppermute(for_peer, "c", [(0, 1), (1, 0)])
    both = (own.astype(jnp.float32) + from_peer.astype(jnp.float32)).astype(jnp.bfloat16)
    tiles = lax.all_to_all(both, "x", 0, 0, tiled=True)
    return jnp.sum(tiles.astype(jnp.float32), axis=0).astype(jnp.bfloat16)


def local(
    residual,
    queries,
    key_pairs,
    values,
    second_weight,
    head_gain,
    out_weight,
    norm_gain,
    up_weight,
    gate_weight,
    conv_weight,
    conv_bias,
    down_weight,
):
    rows = queries.shape[0]
    ff = up_weight.shape[1]
    where = jnp.stack((lax.axis_index("z"), lax.axis_index("y"))).astype(jnp.int32)
    w_rows = up_weight.shape[0]
    width = 2 * ff + ff
    tail = -width % LANES
    cuts = [up_weight, gate_weight, down_weight.T, jnp.zeros((w_rows, tail), jnp.bfloat16)]
    cuts += [queries[i : i + w_rows] for i in range(0, rows, w_rows)]
    row_w = lax.all_gather(jnp.concatenate(cuts, axis=1), "y", axis=0, tiled=True)
    deep = row_w.shape[0]
    shard, q_rows = pl.pallas_call(
        fold_kernel,
        out_shape=[
            jax.ShapeDtypeStruct((deep * width // LANES, LANES), jnp.bfloat16),
            pltpu.VMEM((deep, row_w.shape[1] - width - tail), jnp.bfloat16),
        ],
        in_specs=[VMEM],
        out_specs=[VMEM] * 2,
        name="fold",
    )(pltpu.with_memory_space_constraint(row_w, pltpu.VMEM))
    all_w = lax.all_gather(shard, "z", axis=0, tiled=True)
    all_w = all_w.reshape(-1, *shard.shape)

    kv = jnp.concatenate((key_pairs, values), axis=1)
    last = lax.axis_size("z")
    f5 = shifted(kv, 5, [0, 1, *range(5, last)])
    f11 = shifted(kv, -5, [0, 1, *range(11, last)])
    held = jnp.concatenate((kv, f5, f11), axis=0)
    n1 = shifted(held, 1, range(1, last))
    m1 = shifted(held, -1, [0, *range(4, last)])
    n2 = shifted(n1, 1, range(2, last))
    m2 = shifted(m1, -1, range(3, last))
    e8 = shifted(n2[rows : 2 * rows], 1, range(8, last))
    blocks = [held, n1, m1, n2, m2, e8]
    blocks = [pltpu.with_memory_space_constraint(b, pltpu.VMEM) for b in blocks]
    parts = pl.pallas_call(
        attend_kernel,
        out_shape=pltpu.VMEM((NY * rows, 3 * VD), jnp.bfloat16),
        in_specs=[SMEM] + [VMEM] * (1 + len(blocks)),
        out_specs=VMEM,
        scratch_shapes=[
            pltpu.VMEM((NY * rows, 2 * HD), jnp.bfloat16),
            pltpu.VMEM((len(OFFSETS) * rows, 2 * HD + VD), jnp.bfloat16),
        ],
        name="attend",
    )(where, q_rows, *blocks)
    got = lax.all_to_all(parts.reshape(NY, rows, 3 * VD), "y", 0, 0, tiled=True)
    means = merged(got)
    diff = means[0] - second_weight[0] * means[1]
    scale_inv = lax.rsqrt(jnp.mean(diff * diff, axis=-1, keepdims=True) + eps)
    attended = (diff * scale_inv * head_gain * 0.8).astype(jnp.bfloat16)
    proj = summed_over_tp(
        jnp.dot(attended, out_weight, preferred_element_type=jnp.float32).astype(jnp.bfloat16)
    )
    mid = (residual.astype(jnp.float32) + proj.astype(jnp.float32)).astype(jnp.bfloat16)
    normed_all = lax.all_gather(normalize(mid, norm_gain), TP, axis=0, tiled=True)
    count = lax.axis_size("z") * lax.axis_size("y")
    rim_rows = lax.ppermute(normed_all[rows - 8 :], SP, [(i, i + 1) for i in range(count - 1)])
    d = normed_all.shape[1]
    in_vmem = [
        pltpu.with_memory_space_constraint(v, pltpu.VMEM) for v in (normed_all, rim_rows)
    ]
    ffn = pl.pallas_call(
        ffn_kernel,
        out_shape=pltpu.VMEM((rows, d), jnp.bfloat16),
        in_specs=[VMEM, VMEM, pl.BlockSpec(memory_space=pl.ANY), VMEM, VMEM],
        out_specs=VMEM,
        scratch_shapes=[
            pltpu.VMEM((rows + rim_rows.shape[0], d), jnp.bfloat16),
            pltpu.VMEM((rows + rim_rows.shape[0], 2 * ff), jnp.bfloat16),
            pltpu.VMEM((all_w.shape[0], deep, width + tail), jnp.bfloat16),
            pltpu.VMEM((all_w.shape[0], deep // 2, LANES), jnp.bfloat16),
            pltpu.SemaphoreType.DMA((width // LANES + 1,)),
        ],
        name="ffn",
    )(*in_vmem, all_w, conv_weight, conv_bias)
    ffn_out = summed_over_tp(ffn)
    return (mid.astype(jnp.float32) + ffn_out.astype(jnp.float32)).astype(jnp.bfloat16)


def solution(mesh):
    finer = Mesh(mesh.devices.reshape(NZ, NY, mesh.shape["tp"] // 2, 2), ("z", "y", "x", "c"))
    in_specs = (
        P(SP_TP, None),
        P(SP, TP),
        P(SP, TP),
        P(SP, TP),
        P(TP),
        P(TP),
        P(TP, None),
        P(),
        P(SP, TP),
        P(SP, TP),
        P(None, TP),
        P(TP),
        P(TP, SP),
    )
    out_specs = P(SP_TP, None)
    return jax.shard_map(local, mesh=finer, in_specs=in_specs, out_specs=out_specs, check_vma=False)
```

```python
import jax
import jax.numpy as jnp
from jax import lax
from jax.experimental import pallas as pl
from jax.experimental.pallas import tpu as pltpu
from jax.sharding import Mesh
from jax.sharding import PartitionSpec as P

HD = 64
VD = 128
SP = ("z", "y")
SP_TP = ("z", "y", "x", "c")
TP = ("x", "c")
NZ = 16
NY = 4
eps = 1e-05
neg_fill = -1e30
TILE = 128
LANES = 128
OFFSETS = (0, 5, 11, 1, 6, 12, 15, 4, 10, 2, 7, 13, 14, 3, 9, 8)
CHUNK = 2

VMEM = pl.BlockSpec(memory_space=pltpu.VMEM)
SMEM = pl.BlockSpec(memory_space=pltpu.SMEM)


def shifted(value, steps, targets):
    count = lax.axis_size("z")
    return lax.ppermute(value, "z", [((i - steps) % count, i) for i in targets])


def dot_nt(a, b):
    return lax.dot_general(a, b, (((1,), (1,)), ((), ())), preferred_element_type=jnp.float32)


def row_bias(offsets, rows, z):
    lane = lax.broadcasted_iota(jnp.int32, (1, rows * len(offsets)), 1)
    bias = jnp.zeros(lane.shape, jnp.float32)
    for i, off in enumerate(offsets):
        inside = jnp.logical_and(lane >= i * rows, lane < (i + 1) * rows)
        bias = jnp.where(jnp.logical_and(inside, off > z), neg_fill, bias)
    return bias


def both_maps(q):
    lane = lax.broadcasted_iota(jnp.int32, q.shape, 1)
    q = q * jnp.bfloat16(HD**-0.5)
    zero = jnp.zeros_like(q)
    return jnp.concatenate((jnp.where(lane < HD, q, zero), jnp.where(lane < HD, zero, q)), axis=0)


def packed(columns):
    lane = lax.broadcasted_iota(jnp.int32, (TILE, VD), 1)
    block = jnp.zeros((TILE, VD), jnp.float32)
    for m in range(2):
        for i, v in enumerate(columns):
            column = v[m * TILE : (m + 1) * TILE]
            block = jnp.where(lane == m * len(columns) + i, column, block)
    return block


def attend_kernel(where_ref, *refs):
    query_blocks, blocks, (out_ref, q_ref, kv_ref) = refs[:NY], refs[NY:-3], refs[-3:]
    z = where_ref[0]
    y = where_ref[1]
    rows = kv_ref.shape[0] // len(OFFSETS)
    for behind, block in enumerate(query_blocks):
        first = pl.multiple_of(((y - behind) & (NY - 1)) * rows, rows)
        q_ref[pl.ds(first, rows), :] = block[...]
    filled = 0
    for block in blocks:
        kv_ref[filled : filled + block.shape[0], :] = block[...]
        filled += block.shape[0]
    span = CHUNK * rows
    chunks = [OFFSETS[i : i + CHUNK] for i in range(0, len(OFFSETS), CHUNK)]
    biases = [row_bias(offsets, rows, z) for offsets in chunks]

    @pl.loop(0, NY * rows // TILE)
    def _(t):
        at = pl.multiple_of(t * TILE, TILE)
        q2 = both_maps(q_ref[pl.ds(at, TILE), :])
        scores = []
        for i, bias in enumerate(biases):
            keys = kv_ref[i * span : (i + 1) * span, : 2 * HD]
            scores.append(dot_nt(q2, keys) + bias)
        r = lax.broadcasted_iota(jnp.int32, scores[0].shape, 0)
        r = jnp.where(r >= TILE, r - TILE, r) + at
        k = lax.broadcasted_iota(jnp.int32, scores[0].shape, 1)
        hidden = jnp.logical_and(k < rows, k + y * rows > r)
        scores[0] = jnp.where(hidden, neg_fill, scores[0])
        top = jnp.max(scores[0], axis=1, keepdims=True)
        for s in scores[1:]:
            top = jnp.maximum(top, jnp.max(s, axis=1, keepdims=True))
        total = jnp.zeros((2 * TILE, 1), jnp.float32)
        acc = jnp.zeros((2 * TILE, VD), jnp.float32)
        for i, s in enumerate(scores):
            e = jnp.exp(s - top)
            total = total + jnp.sum(e, axis=1, keepdims=True)
            acc = acc + jnp.dot(
                e.astype(jnp.bfloat16),
                kv_ref[i * span : (i + 1) * span, 2 * HD :],
                preferred_element_type=jnp.float32,
            )
        mean = acc / total
        lse = top + jnp.log(total)
        hi = lse.astype(jnp.bfloat16).astype(jnp.float32)
        mid = (lse - hi).astype(jnp.bfloat16).astype(jnp.float32)
        out_ref[pl.ds(at, TILE), 0:VD] = mean[:TILE].astype(jnp.bfloat16)
        out_ref[pl.ds(at, TILE), VD : 2 * VD] = mean[TILE:].astype(jnp.bfloat16)
        out_ref[pl.ds(at, TILE), 2 * VD : 3 * VD] = packed((hi, mid, lse - hi - mid)).astype(
            jnp.bfloat16
        )


def fold_kernel(rows_ref, out_ref):
    deep = rows_ref.shape[0]
    blocks = out_ref.shape[0] // deep
    for i in range(blocks):
        out_ref[i * deep : (i + 1) * deep, :] = rows_ref[:, i * LANES : (i + 1) * LANES]
    last = rows_ref[:, blocks * LANES : (blocks + 1) * LANES].astype(jnp.float32)
    lane = lax.broadcasted_iota(jnp.int32, (deep // 2, LANES), 1)
    low, high = last[: deep // 2], pltpu.roll(last[deep // 2 :], LANES // 2, 1)
    out_ref[blocks * deep :, :] = jnp.where(lane < LANES // 2, low, high).astype(jnp.bfloat16)


def ffn_kernel(
    rows_ref, rim_ref, w_ref, taps_ref, bias_ref, out_ref, x_ref, acc_ref, held_ref, tail_ref, sems
):
    rows, d = rows_ref.shape
    rim = rim_ref.shape[0]
    ff = bias_ref.shape[0]
    count, deep, _ = held_ref.shape
    full = 3 * ff // LANES
    copies = []
    for i in range(full):
        copies.append(
            pltpu.make_async_copy(
                w_ref.at[:, pl.ds(i * deep, deep), :],
                held_ref.at[:, :, pl.ds(i * LANES, LANES)],
                sems.at[i],
            )
        )
        copies[-1].start()
    copies.append(
        pltpu.make_async_copy(
            w_ref.at[:, pl.ds(full * deep, deep // 2), :], tail_ref, sems.at[full]
        )
    )
    copies[-1].start()
    edges = [*range(0, 2 * ff - 2 * LANES, 4 * LANES), 2 * ff]
    x_ref[:rows, :] = rows_ref[...]
    x_ref[rows:, :] = rim_ref[...]
    for start, end in zip(edges, edges[1:]):
        for i in range(start // LANES, end // LANES):
            copies[i].wait()
        acc_ref[:, start:end] = jnp.dot(
            x_ref[...],
            held_ref[:, :, start:end].reshape(d, end - start),
            preferred_element_type=jnp.float32,
        ).astype(jnp.bfloat16)
    up = acc_ref[:, :ff].astype(jnp.float32)
    gate = acc_ref[:rows, ff : 2 * ff].astype(jnp.float32)
    before = up[rows:]
    up = up[:rows]
    at = lax.broadcasted_iota(jnp.int32, up.shape, 0)
    one = jnp.where(at == 0, before[rim - 1 : rim], pltpu.roll(up, 1, 0))
    two = pltpu.roll(up, 2, 0)
    two = jnp.where(at == 0, before[rim - 2 : rim - 1], two)
    two = jnp.where(at == 1, before[rim - 1 : rim], two)
    conv = bias_ref[...].reshape(1, ff) + taps_ref[0:1] * two + taps_ref[1:2] * one + taps_ref[2:3] * up
    hidden = (conv / (1.0 + jnp.exp(-conv)) * gate).astype(jnp.bfloat16)
    for copy in copies[2 * ff // LANES :]:
        copy.wait()
    tail = tail_ref[...].reshape(count * deep // 2, LANES).astype(jnp.float32)
    pair = (tail, pltpu.roll(tail, LANES // 2, 1))
    for i, half in enumerate(pair):
        block = half.astype(jnp.bfloat16).reshape(count, deep // 2, LANES)
        held_ref[:, i * deep // 2 : (i + 1) * deep // 2, full * LANES :] = block
    down = held_ref[:, :, 2 * ff : 3 * ff].reshape(d, ff)
    out_ref[...] = dot_nt(hidden, down).astype(jnp.bfloat16)


def merged(got):
    got = got.astype(jnp.float32)
    means = []
    for m in range(2):
        stat = got[:, :, 2 * VD + 3 * m : 2 * VD + 3 * m + 3]
        lse = stat[..., 0:1] + stat[..., 1:2] + stat[..., 2:3]
        share = jnp.exp(lse - jnp.max(lse, axis=0, keepdims=True))
        acc = jnp.sum(share * got[:, :, m * VD : (m + 1) * VD], axis=0)
        means.append(acc / jnp.sum(share, axis=0))
    return means


def normalize(rows_in, gain):
    values_f = rows_in.astype(jnp.float32)
    scale_inv = lax.rsqrt(jnp.mean(values_f * values_f, axis=-1, keepdims=True) + eps)
    return (values_f * scale_inv * gain).astype(jnp.bfloat16)


def summed_over_tp(shard):
    core = lax.axis_index("c")
    count = lax.axis_size(TP)
    cut = shard.reshape(count // 2, 2, shard.shape[0] // count, shard.shape[1])
    own = jnp.where(core == 0, cut[:, 0], cut[:, 1])
    for_peer = jnp.where(core == 0, cut[:, 1], cut[:, 0])
    from_peer = lax.ppermute(for_peer, "c", [(0, 1), (1, 0)])
    both = (own.astype(jnp.float32) + from_peer.astype(jnp.float32)).astype(jnp.bfloat16)
    tiles = lax.all_to_all(both, "x", 0, 0, tiled=True)
    return jnp.sum(tiles.astype(jnp.float32), axis=0).astype(jnp.bfloat16)


def local(
    residual,
    queries,
    key_pairs,
    values,
    second_weight,
    head_gain,
    out_weight,
    norm_gain,
    up_weight,
    gate_weight,
    conv_weight,
    conv_bias,
    down_weight,
):
    rows = queries.shape[0]
    ff = up_weight.shape[1]
    where = jnp.stack((lax.axis_index("z"), lax.axis_index("y"))).astype(jnp.int32)
    w_rows = up_weight.shape[0]
    width = 2 * ff + ff
    tail = -width % LANES
    cuts = [up_weight, gate_weight, down_weight.T, jnp.zeros((w_rows, tail), jnp.bfloat16)]
    row_w = lax.all_gather(jnp.concatenate(cuts, axis=1), "y", axis=0, tiled=True)
    deep = row_w.shape[0]
    shard = pl.pallas_call(
        fold_kernel,
        out_shape=jax.ShapeDtypeStruct((deep * width // LANES, LANES), jnp.bfloat16),
        in_specs=[VMEM],
        out_specs=VMEM,
        name="fold",
    )(pltpu.with_memory_space_constraint(row_w, pltpu.VMEM))
    all_w = lax.all_gather(shard, "z", axis=0, tiled=True)
    all_w = all_w.reshape(-1, *shard.shape)

    kv = jnp.concatenate((key_pairs, values), axis=1)
    last = lax.axis_size("z")
    f5 = shifted(kv, 5, [0, 1, *range(5, last)])
    f11 = shifted(kv, -5, [0, 1, *range(11, last)])
    query_blocks = [queries]
    for behind in range(1, NY):
        pairs = [((i - behind) % NY, i) for i in range(NY)]
        query_blocks.append(lax.ppermute(queries, "y", pairs))
    held = jnp.concatenate((kv, f5, f11), axis=0)
    n1 = shifted(held, 1, range(1, last))
    m1 = shifted(held, -1, [0, *range(4, last)])
    n2 = shifted(n1, 1, range(2, last))
    m2 = shifted(m1, -1, range(3, last))
    e8 = shifted(n2[rows : 2 * rows], 1, range(8, last))
    blocks = [held, n1, m1, n2, m2, e8]
    blocks = query_blocks + blocks
    blocks = [pltpu.with_memory_space_constraint(b, pltpu.VMEM) for b in blocks]
    parts = pl.pallas_call(
        attend_kernel,
        out_shape=pltpu.VMEM((NY * rows, 3 * VD), jnp.bfloat16),
        in_specs=[SMEM] + [VMEM] * len(blocks),
        out_specs=VMEM,
        scratch_shapes=[
            pltpu.VMEM((NY * rows, 2 * HD), jnp.bfloat16),
            pltpu.VMEM((len(OFFSETS) * rows, 2 * HD + VD), jnp.bfloat16),
        ],
        name="attend",
    )(where, *blocks)
    got = lax.all_to_all(parts.reshape(NY, rows, 3 * VD), "y", 0, 0, tiled=True)
    means = merged(got)
    diff = means[0] - second_weight[0] * means[1]
    scale_inv = lax.rsqrt(jnp.mean(diff * diff, axis=-1, keepdims=True) + eps)
    attended = (diff * scale_inv * head_gain * 0.8).astype(jnp.bfloat16)
    proj = summed_over_tp(
        jnp.dot(attended, out_weight, preferred_element_type=jnp.float32).astype(jnp.bfloat16)
    )
    mid = (residual.astype(jnp.float32) + proj.astype(jnp.float32)).astype(jnp.bfloat16)
    normed_all = lax.all_gather(normalize(mid, norm_gain), TP, axis=0, tiled=True)
    count = lax.axis_size("z") * lax.axis_size("y")
    rim_rows = lax.ppermute(normed_all[rows - 8 :], SP, [(i, i + 1) for i in range(count - 1)])
    d = normed_all.shape[1]
    in_vmem = [
        pltpu.with_memory_space_constraint(v, pltpu.VMEM) for v in (normed_all, rim_rows)
    ]
    ffn = pl.pallas_call(
        ffn_kernel,
        out_shape=pltpu.VMEM((rows, d), jnp.bfloat16),
        in_specs=[VMEM, VMEM, pl.BlockSpec(memory_space=pl.ANY), VMEM, VMEM],
        out_specs=VMEM,
        scratch_shapes=[
            pltpu.VMEM((rows + rim_rows.shape[0], d), jnp.bfloat16),
            pltpu.VMEM((rows + rim_rows.shape[0], 2 * ff), jnp.bfloat16),
            pltpu.VMEM((all_w.shape[0], deep, width + tail), jnp.bfloat16),
            pltpu.VMEM((all_w.shape[0], deep // 2, LANES), jnp.bfloat16),
            pltpu.SemaphoreType.DMA((width // LANES + 1,)),
        ],
        name="ffn",
    )(*in_vmem, all_w, conv_weight, conv_bias)
    ffn_out = summed_over_tp(ffn)
    return (mid.astype(jnp.float32) + ffn_out.astype(jnp.float32)).astype(jnp.bfloat16)


def solution(mesh):
    finer = Mesh(mesh.devices.reshape(NZ, NY, mesh.shape["tp"] // 2, 2), ("z", "y", "x", "c"))
    in_specs = (
        P(SP_TP, None),
        P(SP, TP),
        P(SP, TP),
        P(SP, TP),
        P(TP),
        P(TP),
        P(TP, None),
        P(),
        P(SP, TP),
        P(SP, TP),
        P(None, TP),
        P(TP),
        P(TP, SP),
    )
    out_specs = P(SP_TP, None)
    return jax.shard_map(local, mesh=finer, in_specs=in_specs, out_specs=out_specs, check_vma=False)
```

```python
import jax
import jax.numpy as jnp
from jax import lax
from jax.experimental import pallas as pl
from jax.experimental.pallas import tpu as pltpu
from jax.sharding import Mesh
from jax.sharding import PartitionSpec as P

HD = 64
VD = 128
SP = ("z", "y")
SP_TP = ("z", "y", "x", "c")
TP = ("x", "c")
NZ = 16
NY = 4
eps = 1e-05
neg_fill = -1e30
TILE = 128
LANES = 128
OFFSETS = (0, 5, 11, 1, 6, 12, 15, 4, 10, 2, 7, 13, 14, 3, 9, 8)
CHUNK = 2

VMEM = pl.BlockSpec(memory_space=pltpu.VMEM)
SMEM = pl.BlockSpec(memory_space=pltpu.SMEM)


def shifted(value, steps, targets):
    count = lax.axis_size("z")
    return lax.ppermute(value, "z", [((i - steps) % count, i) for i in targets])


def dot_nt(a, b):
    return lax.dot_general(a, b, (((1,), (1,)), ((), ())), preferred_element_type=jnp.float32)


def row_bias(offsets, rows, z):
    lane = lax.broadcasted_iota(jnp.int32, (1, rows * len(offsets)), 1)
    bias = jnp.zeros(lane.shape, jnp.float32)
    for i, off in enumerate(offsets):
        inside = jnp.logical_and(lane >= i * rows, lane < (i + 1) * rows)
        bias = jnp.where(jnp.logical_and(inside, off > z), neg_fill, bias)
    return bias


def both_maps(q):
    lane = lax.broadcasted_iota(jnp.int32, q.shape, 1)
    q = q * jnp.bfloat16(HD**-0.5)
    zero = jnp.zeros_like(q)
    return jnp.concatenate((jnp.where(lane < HD, q, zero), jnp.where(lane < HD, zero, q)), axis=0)


def packed(columns):
    lane = lax.broadcasted_iota(jnp.int32, (TILE, VD), 1)
    block = jnp.zeros((TILE, VD), jnp.float32)
    for m in range(2):
        for i, v in enumerate(columns):
            column = v[m * TILE : (m + 1) * TILE]
            block = jnp.where(lane == m * len(columns) + i, column, block)
    return block


def attend_kernel(where_ref, *refs):
    query_blocks, blocks, (out_ref, q_ref, kv_ref) = refs[:NY], refs[NY:-3], refs[-3:]
    z = where_ref[0]
    y = where_ref[1]
    rows = kv_ref.shape[0] // len(OFFSETS)
    for behind, block in enumerate(query_blocks):
        first = pl.multiple_of(((y - behind) & (NY - 1)) * rows, rows)
        q_ref[pl.ds(first, rows), :] = block[...]
    filled = 0
    for block in blocks:
        kv_ref[filled : filled + block.shape[0], :] = block[...]
        filled += block.shape[0]
    span = CHUNK * rows
    chunks = [OFFSETS[i : i + CHUNK] for i in range(0, len(OFFSETS), CHUNK)]
    biases = [row_bias(offsets, rows, z) for offsets in chunks]

    @pl.loop(0, NY * rows // TILE)
    def _(t):
        at = pl.multiple_of(t * TILE, TILE)
        q2 = both_maps(q_ref[pl.ds(at, TILE), :])
        scores = []
        for i, bias in enumerate(biases):
            keys = kv_ref[i * span : (i + 1) * span, : 2 * HD]
            scores.append(dot_nt(q2, keys) + bias)
        r = lax.broadcasted_iota(jnp.int32, scores[0].shape, 0)
        r = jnp.where(r >= TILE, r - TILE, r) + at
        k = lax.broadcasted_iota(jnp.int32, scores[0].shape, 1)
        hidden = jnp.logical_and(k < rows, k + y * rows > r)
        scores[0] = jnp.where(hidden, neg_fill, scores[0])
        top = jnp.max(scores[0], axis=1, keepdims=True)
        for s in scores[1:]:
            top = jnp.maximum(top, jnp.max(s, axis=1, keepdims=True))
        total = jnp.zeros((2 * TILE, 1), jnp.float32)
        acc = jnp.zeros((2 * TILE, VD), jnp.float32)
        for i, s in enumerate(scores):
            e = jnp.exp(s - top)
            total = total + jnp.sum(e, axis=1, keepdims=True)
            acc = acc + jnp.dot(
                e.astype(jnp.bfloat16),
                kv_ref[i * span : (i + 1) * span, 2 * HD :],
                preferred_element_type=jnp.float32,
            )
        mean = acc / total
        lse = top + jnp.log(total)
        hi = lse.astype(jnp.bfloat16).astype(jnp.float32)
        mid = (lse - hi).astype(jnp.bfloat16).astype(jnp.float32)
        out_ref[pl.ds(at, TILE), 0:VD] = mean[:TILE].astype(jnp.bfloat16)
        out_ref[pl.ds(at, TILE), VD : 2 * VD] = mean[TILE:].astype(jnp.bfloat16)
        out_ref[pl.ds(at, TILE), 2 * VD : 3 * VD] = packed((hi, mid, lse - hi - mid)).astype(
            jnp.bfloat16
        )


def fold_kernel(rows_ref, out_ref):
    deep = rows_ref.shape[0]
    blocks = out_ref.shape[0] // deep
    for i in range(blocks):
        out_ref[i * deep : (i + 1) * deep, :] = rows_ref[:, i * LANES : (i + 1) * LANES]
    last = rows_ref[:, blocks * LANES : (blocks + 1) * LANES].astype(jnp.float32)
    lane = lax.broadcasted_iota(jnp.int32, (deep // 2, LANES), 1)
    low, high = last[: deep // 2], pltpu.roll(last[deep // 2 :], LANES // 2, 1)
    out_ref[blocks * deep :, :] = jnp.where(lane < LANES // 2, low, high).astype(jnp.bfloat16)


def ffn_kernel(
    rows_ref, rim_ref, w_ref, taps_ref, bias_ref, out_ref, x_ref, acc_ref, held_ref, tail_ref, sems
):
    rows, d = rows_ref.shape
    rim = rim_ref.shape[0]
    ff = bias_ref.shape[0]
    count, deep, _ = held_ref.shape
    full = 3 * ff // LANES
    copies = []
    for i in range(full):
        copies.append(
            pltpu.make_async_copy(
                w_ref.at[:, pl.ds(i * deep, deep), :],
                held_ref.at[:, :, pl.ds(i * LANES, LANES)],
                sems.at[i],
            )
        )
        copies[-1].start()
    copies.append(
        pltpu.make_async_copy(
            w_ref.at[:, pl.ds(full * deep, deep // 2), :], tail_ref, sems.at[full]
        )
    )
    copies[-1].start()
    edges = [*range(0, 2 * ff - 2 * LANES, 4 * LANES), 2 * ff]
    x_ref[:rows, :] = rows_ref[...]
    x_ref[rows:, :] = rim_ref[...]
    for start, end in zip(edges, edges[1:]):
        for i in range(start // LANES, end // LANES):
            copies[i].wait()
        acc_ref[:, start:end] = jnp.dot(
            x_ref[...],
            held_ref[:, :, start:end].reshape(d, end - start),
            preferred_element_type=jnp.float32,
        ).astype(jnp.bfloat16)
    up = acc_ref[:, :ff].astype(jnp.float32)
    gate = acc_ref[:rows, ff : 2 * ff].astype(jnp.float32)
    before = up[rows:]
    up = up[:rows]
    at = lax.broadcasted_iota(jnp.int32, up.shape, 0)
    one = jnp.where(at == 0, before[rim - 1 : rim], pltpu.roll(up, 1, 0))
    two = pltpu.roll(up, 2, 0)
    two = jnp.where(at == 0, before[rim - 2 : rim - 1], two)
    two = jnp.where(at == 1, before[rim - 1 : rim], two)
    conv = bias_ref[...].reshape(1, ff) + taps_ref[0:1] * two + taps_ref[1:2] * one + taps_ref[2:3] * up
    hidden = (conv / (1.0 + jnp.exp(-conv)) * gate).astype(jnp.bfloat16)
    for copy in copies[2 * ff // LANES :]:
        copy.wait()
    tail = tail_ref[...].reshape(count * deep // 2, LANES).astype(jnp.float32)
    pair = (tail, pltpu.roll(tail, LANES // 2, 1))
    for i, half in enumerate(pair):
        block = half.astype(jnp.bfloat16).reshape(count, deep // 2, LANES)
        held_ref[:, i * deep // 2 : (i + 1) * deep // 2, full * LANES :] = block
    down = held_ref[:, :, 2 * ff : 3 * ff].reshape(d, ff)
    out_ref[...] = dot_nt(hidden, down).astype(jnp.bfloat16)


def merged(got):
    got = got.astype(jnp.float32)
    means = []
    for m in range(2):
        stat = got[:, :, 2 * VD + 3 * m : 2 * VD + 3 * m + 3]
        lse = stat[..., 0:1] + stat[..., 1:2] + stat[..., 2:3]
        share = jnp.exp(lse - jnp.max(lse, axis=0, keepdims=True))
        acc = jnp.sum(share * got[:, :, m * VD : (m + 1) * VD], axis=0)
        means.append(acc / jnp.sum(share, axis=0))
    return means


def normalize(rows_in, gain):
    values_f = rows_in.astype(jnp.float32)
    scale_inv = lax.rsqrt(jnp.mean(values_f * values_f, axis=-1, keepdims=True) + eps)
    return (values_f * scale_inv * gain).astype(jnp.bfloat16)


def summed_over_tp(shard):
    core = lax.axis_index("c")
    count = lax.axis_size(TP)
    cut = shard.reshape(count // 2, 2, shard.shape[0] // count, shard.shape[1])
    own = jnp.where(core == 0, cut[:, 0], cut[:, 1])
    for_peer = jnp.where(core == 0, cut[:, 1], cut[:, 0])
    from_peer = lax.ppermute(for_peer, "c", [(0, 1), (1, 0)])
    both = (own.astype(jnp.float32) + from_peer.astype(jnp.float32)).astype(jnp.bfloat16)
    tiles = lax.all_to_all(both, "x", 0, 0, tiled=True)
    return jnp.sum(tiles.astype(jnp.float32), axis=0).astype(jnp.bfloat16)


def local(
    residual,
    queries,
    key_pairs,
    values,
    second_weight,
    head_gain,
    out_weight,
    norm_gain,
    up_weight,
    gate_weight,
    conv_weight,
    conv_bias,
    down_weight,
):
    rows = queries.shape[0]
    ff = up_weight.shape[1]
    where = jnp.stack((lax.axis_index("z"), lax.axis_index("y"))).astype(jnp.int32)
    w_rows = up_weight.shape[0]
    width = 2 * ff + ff
    tail = -width % LANES
    cuts = [up_weight, gate_weight, down_weight.T, jnp.zeros((w_rows, tail), jnp.bfloat16)]
    row_w = lax.all_gather(jnp.concatenate(cuts, axis=1), "y", axis=0, tiled=True)
    deep = row_w.shape[0]
    shard = pl.pallas_call(
        fold_kernel,
        out_shape=jax.ShapeDtypeStruct((deep * width // LANES, LANES), jnp.bfloat16),
        in_specs=[VMEM],
        out_specs=VMEM,
        name="fold",
    )(pltpu.with_memory_space_constraint(row_w, pltpu.VMEM))
    all_w = lax.all_gather(shard, "z", axis=0, tiled=True)
    all_w = all_w.reshape(-1, *shard.shape)

    kv = jnp.concatenate((key_pairs, values), axis=1)
    last = lax.axis_size("z")
    f5 = shifted(kv, 5, [0, 1, *range(5, last)])
    f11 = shifted(kv, -5, [0, 1, *range(11, last)])
    query_blocks = [queries]
    for behind in range(1, NY):
        pairs = [((i - behind) % NY, i) for i in range(NY)]
        query_blocks.append(lax.ppermute(queries, "y", pairs))
    held = jnp.concatenate((kv, f5, f11), axis=0)
    n1 = shifted(held, 1, range(1, last))
    m1 = shifted(held, -1, [0, *range(4, last)])
    n2 = shifted(n1, 1, range(2, last))
    m2 = shifted(m1, -1, range(3, last))
    e8 = shifted(n2[rows : 2 * rows], 1, range(8, last))
    blocks = [held, n1, m1, n2, m2, e8]
    blocks = query_blocks + blocks
    blocks = [pltpu.with_memory_space_constraint(b, pltpu.VMEM) for b in blocks]
    parts = pl.pallas_call(
        attend_kernel,
        out_shape=pltpu.VMEM((NY * rows, 3 * VD), jnp.bfloat16),
        in_specs=[SMEM] + [VMEM] * len(blocks),
        out_specs=VMEM,
        scratch_shapes=[
            pltpu.VMEM((NY * rows, 2 * HD), jnp.bfloat16),
            pltpu.VMEM((len(OFFSETS) * rows, 2 * HD + VD), jnp.bfloat16),
        ],
        name="attend",
    )(where, *blocks)
    got = lax.all_to_all(parts.reshape(NY, rows, 3 * VD), "y", 0, 0, tiled=True)
    means = merged(got)
    diff = means[0] - second_weight[0] * means[1]
    scale_inv = lax.rsqrt(jnp.mean(diff * diff, axis=-1, keepdims=True) + eps)
    attended = (diff * scale_inv * head_gain * 0.8).astype(jnp.bfloat16)
    proj = summed_over_tp(
        jnp.dot(attended, out_weight, preferred_element_type=jnp.float32).astype(jnp.bfloat16)
    )
    mid = (residual.astype(jnp.float32) + proj.astype(jnp.float32)).astype(jnp.bfloat16)
    normed_all = lax.all_gather(normalize(mid, norm_gain), TP, axis=0, tiled=True)
    count = lax.axis_size("z") * lax.axis_size("y")
    rim_rows = lax.ppermute(normed_all[rows - 8 :], SP, [(i, i + 1) for i in range(count - 1)])
    d = normed_all.shape[1]
    in_vmem = [
        pltpu.with_memory_space_constraint(v, pltpu.VMEM) for v in (normed_all, rim_rows)
    ]
    ffn = pl.pallas_call(
        ffn_kernel,
        out_shape=pltpu.VMEM((rows, d), jnp.bfloat16),
        in_specs=[VMEM, VMEM, pl.BlockSpec(memory_space=pl.ANY), VMEM, VMEM],
        out_specs=VMEM,
        scratch_shapes=[
            pltpu.VMEM((rows + rim_rows.shape[0], d), jnp.bfloat16),
            pltpu.VMEM((rows + rim_rows.shape[0], 2 * ff), jnp.bfloat16),
            pltpu.VMEM((all_w.shape[0], deep, width + tail), jnp.bfloat16),
            pltpu.VMEM((all_w.shape[0], deep // 2, LANES), jnp.bfloat16),
            pltpu.SemaphoreType.DMA((width // LANES + 1,)),
        ],
        compiler_params=pltpu.CompilerParams(vmem_limit_bytes=40 * 2**20),
        name="ffn",
    )(*in_vmem, pltpu.with_memory_space_constraint(all_w, pltpu.HBM), conv_weight, conv_bias)
    ffn_out = summed_over_tp(ffn)
    return (mid.astype(jnp.float32) + ffn_out.astype(jnp.float32)).astype(jnp.bfloat16)


def solution(mesh):
    finer = Mesh(mesh.devices.reshape(NZ, NY, mesh.shape["tp"] // 2, 2), ("z", "y", "x", "c"))
    in_specs = (
        P(SP_TP, None),
        P(SP, TP),
        P(SP, TP),
        P(SP, TP),
        P(TP),
        P(TP),
        P(TP, None),
        P(),
        P(SP, TP),
        P(SP, TP),
        P(None, TP),
        P(TP),
        P(TP, SP),
    )
    out_specs = P(SP_TP, None)
    return jax.shard_map(local, mesh=finer, in_specs=in_specs, out_specs=out_specs, check_vma=False)
```

```python
import jax
import jax.numpy as jnp
from jax import lax
from jax.experimental import pallas as pl
from jax.experimental.pallas import tpu as pltpu
from jax.sharding import Mesh
from jax.sharding import PartitionSpec as P

HD = 64
VD = 128
SP = ("z", "y")
SP_TP = ("z", "y", "x", "c")
TP = ("x", "c")
NZ = 16
NY = 4
eps = 1e-05
neg_fill = -1e30
TILE = 128
LANES = 128
OFFSETS = (0, 5, 11, 1, 6, 12, 15, 4, 10, 2, 7, 13, 14, 3, 9, 8)
CHUNK = 2

VMEM = pl.BlockSpec(memory_space=pltpu.VMEM)
SMEM = pl.BlockSpec(memory_space=pltpu.SMEM)


def shifted(value, steps, targets):
    count = lax.axis_size("z")
    return lax.ppermute(value, "z", [((i - steps) % count, i) for i in targets])


def dot_nt(a, b):
    return lax.dot_general(a, b, (((1,), (1,)), ((), ())), preferred_element_type=jnp.float32)


def row_bias(offsets, rows, z):
    lane = lax.broadcasted_iota(jnp.int32, (1, rows * len(offsets)), 1)
    bias = jnp.zeros(lane.shape, jnp.float32)
    for i, off in enumerate(offsets):
        inside = jnp.logical_and(lane >= i * rows, lane < (i + 1) * rows)
        bias = jnp.where(jnp.logical_and(inside, off > z), neg_fill, bias)
    return bias


def both_maps(q):
    lane = lax.broadcasted_iota(jnp.int32, q.shape, 1)
    q = q * jnp.bfloat16(HD**-0.5)
    zero = jnp.zeros_like(q)
    return jnp.concatenate((jnp.where(lane < HD, q, zero), jnp.where(lane < HD, zero, q)), axis=0)


def packed(columns):
    lane = lax.broadcasted_iota(jnp.int32, (TILE, VD), 1)
    block = jnp.zeros((TILE, VD), jnp.float32)
    for m in range(2):
        for i, v in enumerate(columns):
            column = v[m * TILE : (m + 1) * TILE]
            block = jnp.where(lane == m * len(columns) + i, column, block)
    return block


def attend_kernel(where_ref, *refs):
    query_blocks, blocks, (out_ref, q_ref, kv_ref) = refs[:NY], refs[NY:-3], refs[-3:]
    z = where_ref[0]
    y = where_ref[1]
    rows = kv_ref.shape[0] // len(OFFSETS)
    for behind, block in enumerate(query_blocks):
        first = pl.multiple_of(((y - behind) & (NY - 1)) * rows, rows)
        q_ref[pl.ds(first, rows), :] = block[...]
    filled = 0
    for block in blocks:
        kv_ref[filled : filled + block.shape[0], :] = block[...]
        filled += block.shape[0]
    span = CHUNK * rows
    chunks = [OFFSETS[i : i + CHUNK] for i in range(0, len(OFFSETS), CHUNK)]
    biases = [row_bias(offsets, rows, z) for offsets in chunks]

    @pl.loop(0, NY * rows // TILE)
    def _(t):
        at = pl.multiple_of(t * TILE, TILE)
        q2 = both_maps(q_ref[pl.ds(at, TILE), :])
        scores = []
        for i, bias in enumerate(biases):
            keys = kv_ref[i * span : (i + 1) * span, : 2 * HD]
            scores.append(dot_nt(q2, keys) + bias)
        r = lax.broadcasted_iota(jnp.int32, scores[0].shape, 0)
        r = jnp.where(r >= TILE, r - TILE, r) + at
        k = lax.broadcasted_iota(jnp.int32, scores[0].shape, 1)
        hidden = jnp.logical_and(k < rows, k + y * rows > r)
        scores[0] = jnp.where(hidden, neg_fill, scores[0])
        top = jnp.max(scores[0], axis=1, keepdims=True)
        for s in scores[1:]:
            top = jnp.maximum(top, jnp.max(s, axis=1, keepdims=True))
        total = jnp.zeros((2 * TILE, 1), jnp.float32)
        acc = jnp.zeros((2 * TILE, VD), jnp.float32)
        for i, s in enumerate(scores):
            e = jnp.exp(s - top)
            total = total + jnp.sum(e, axis=1, keepdims=True)
            acc = acc + jnp.dot(
                e.astype(jnp.bfloat16),
                kv_ref[i * span : (i + 1) * span, 2 * HD :],
                preferred_element_type=jnp.float32,
            )
        mean = acc / total
        lse = top + jnp.log(total)
        hi = lse.astype(jnp.bfloat16).astype(jnp.float32)
        mid = (lse - hi).astype(jnp.bfloat16).astype(jnp.float32)
        out_ref[pl.ds(at, TILE), 0:VD] = mean[:TILE].astype(jnp.bfloat16)
        out_ref[pl.ds(at, TILE), VD : 2 * VD] = mean[TILE:].astype(jnp.bfloat16)
        out_ref[pl.ds(at, TILE), 2 * VD : 3 * VD] = packed((hi, mid, lse - hi - mid)).astype(
            jnp.bfloat16
        )


def fold_kernel(rows_ref, out_ref):
    deep = rows_ref.shape[0]
    blocks = out_ref.shape[0] // deep
    for i in range(blocks):
        out_ref[i * deep : (i + 1) * deep, :] = rows_ref[:, i * LANES : (i + 1) * LANES]
    last = rows_ref[:, blocks * LANES : (blocks + 1) * LANES].astype(jnp.float32)
    lane = lax.broadcasted_iota(jnp.int32, (deep // 2, LANES), 1)
    low, high = last[: deep // 2], pltpu.roll(last[deep // 2 :], LANES // 2, 1)
    out_ref[blocks * deep :, :] = jnp.where(lane < LANES // 2, low, high).astype(jnp.bfloat16)


def ffn_kernel(
    rows_ref, rim_ref, w_ref, taps_ref, bias_ref, out_ref, x_ref, acc_ref, held_ref, tail_ref, sems
):
    rows, d = rows_ref.shape
    rim = rim_ref.shape[0]
    ff = bias_ref.shape[0]
    count, deep, _ = held_ref.shape
    full = 3 * ff // LANES
    copies = []
    for i in range(full):
        copies.append(
            pltpu.make_async_copy(
                w_ref.at[:, pl.ds(i * deep, deep), :],
                held_ref.at[:, :, pl.ds(i * LANES, LANES)],
                sems.at[i],
            )
        )
        copies[-1].start()
    copies.append(
        pltpu.make_async_copy(
            w_ref.at[:, pl.ds(full * deep, deep // 2), :], tail_ref, sems.at[full]
        )
    )
    copies[-1].start()
    edges = [*range(0, 2 * ff - 2 * LANES, 4 * LANES), 2 * ff]
    x_ref[:rows, :] = rows_ref[...]
    x_ref[rows:, :] = rim_ref[...]
    for start, end in zip(edges, edges[1:]):
        for i in range(start // LANES, end // LANES):
            copies[i].wait()
        acc_ref[:, start:end] = jnp.dot(
            x_ref[...],
            held_ref[:, :, start:end].reshape(d, end - start),
            preferred_element_type=jnp.float32,
        ).astype(jnp.bfloat16)
    up = acc_ref[:, :ff].astype(jnp.float32)
    gate = acc_ref[:rows, ff : 2 * ff].astype(jnp.float32)
    before = up[rows:]
    up = up[:rows]
    at = lax.broadcasted_iota(jnp.int32, up.shape, 0)
    one = jnp.where(at == 0, before[rim - 1 : rim], pltpu.roll(up, 1, 0))
    two = pltpu.roll(up, 2, 0)
    two = jnp.where(at == 0, before[rim - 2 : rim - 1], two)
    two = jnp.where(at == 1, before[rim - 1 : rim], two)
    conv = bias_ref[...].reshape(1, ff) + taps_ref[0:1] * two + taps_ref[1:2] * one + taps_ref[2:3] * up
    hidden = (conv / (1.0 + jnp.exp(-conv)) * gate).astype(jnp.bfloat16)
    for copy in copies[2 * ff // LANES :]:
        copy.wait()
    tail = tail_ref[...].reshape(count * deep // 2, LANES).astype(jnp.float32)
    pair = (tail, pltpu.roll(tail, LANES // 2, 1))
    for i, half in enumerate(pair):
        block = half.astype(jnp.bfloat16).reshape(count, deep // 2, LANES)
        held_ref[:, i * deep // 2 : (i + 1) * deep // 2, full * LANES :] = block
    down = held_ref[:, :, 2 * ff : 3 * ff].reshape(d, ff)
    out_ref[...] = dot_nt(hidden, down).astype(jnp.bfloat16)


def merged(got):
    got = got.astype(jnp.float32)
    means = []
    for m in range(2):
        stat = got[:, :, 2 * VD + 3 * m : 2 * VD + 3 * m + 3]
        lse = stat[..., 0:1] + stat[..., 1:2] + stat[..., 2:3]
        share = jnp.exp(lse - jnp.max(lse, axis=0, keepdims=True))
        acc = jnp.sum(share * got[:, :, m * VD : (m + 1) * VD], axis=0)
        means.append(acc / jnp.sum(share, axis=0))
    return means


def normalize(rows_in, gain):
    values_f = rows_in.astype(jnp.float32)
    scale_inv = lax.rsqrt(jnp.mean(values_f * values_f, axis=-1, keepdims=True) + eps)
    return (values_f * scale_inv * gain).astype(jnp.bfloat16)


def summed_over_tp(shard):
    core = lax.axis_index("c")
    count = lax.axis_size(TP)
    cut = shard.reshape(count // 2, 2, shard.shape[0] // count, shard.shape[1])
    own = jnp.where(core == 0, cut[:, 0], cut[:, 1])
    for_peer = jnp.where(core == 0, cut[:, 1], cut[:, 0])
    from_peer = lax.ppermute(for_peer, "c", [(0, 1), (1, 0)])
    both = (own.astype(jnp.float32) + from_peer.astype(jnp.float32)).astype(jnp.bfloat16)
    tiles = lax.all_to_all(both, "x", 0, 0, tiled=True)
    return jnp.sum(tiles.astype(jnp.float32), axis=0).astype(jnp.bfloat16)


def local(
    residual,
    queries,
    key_pairs,
    values,
    second_weight,
    head_gain,
    out_weight,
    norm_gain,
    up_weight,
    gate_weight,
    conv_weight,
    conv_bias,
    down_weight,
):
    rows = queries.shape[0]
    ff = up_weight.shape[1]
    where = jnp.stack((lax.axis_index("z"), lax.axis_index("y"))).astype(jnp.int32)
    w_rows = up_weight.shape[0]
    width = 2 * ff + ff
    tail = -width % LANES
    cuts = [up_weight, gate_weight, down_weight.T, jnp.zeros((w_rows, tail), jnp.bfloat16)]
    row_w = lax.all_gather(jnp.concatenate(cuts, axis=1), "y", axis=0, tiled=True)
    deep = row_w.shape[0]
    shard = pl.pallas_call(
        fold_kernel,
        out_shape=jax.ShapeDtypeStruct((deep * width // LANES, LANES), jnp.bfloat16),
        in_specs=[VMEM],
        out_specs=VMEM,
        name="fold",
    )(pltpu.with_memory_space_constraint(row_w, pltpu.VMEM))
    all_w = lax.all_gather(shard, "z", axis=0, tiled=True)
    all_w = all_w.reshape(-1, *shard.shape)

    kv = jnp.concatenate((key_pairs, values), axis=1)
    last = lax.axis_size("z")
    f5 = shifted(kv, 5, [0, 1, *range(5, last)])
    f11 = shifted(kv, -5, [0, 1, *range(11, last)])
    query_blocks = [queries]
    for behind in range(1, NY):
        pairs = [((i - behind) % NY, i) for i in range(NY)]
        query_blocks.append(lax.ppermute(queries, "y", pairs))
    f5, f11, query_blocks[1] = lax.optimization_barrier((f5, f11, query_blocks[1]))
    held = jnp.concatenate((kv, f5, f11), axis=0)
    n1 = shifted(held, 1, range(1, last))
    m1 = shifted(held, -1, [0, *range(4, last)])
    n2 = shifted(n1, 1, range(2, last))
    m2 = shifted(m1, -1, range(3, last))
    e8 = shifted(n2[rows : 2 * rows], 1, range(8, last))
    blocks = [held, n1, m1, n2, m2, e8]
    blocks = query_blocks + blocks
    blocks = [pltpu.with_memory_space_constraint(b, pltpu.VMEM) for b in blocks]
    parts = pl.pallas_call(
        attend_kernel,
        out_shape=pltpu.VMEM((NY * rows, 3 * VD), jnp.bfloat16),
        in_specs=[SMEM] + [VMEM] * len(blocks),
        out_specs=VMEM,
        scratch_shapes=[
            pltpu.VMEM((NY * rows, 2 * HD), jnp.bfloat16),
            pltpu.VMEM((len(OFFSETS) * rows, 2 * HD + VD), jnp.bfloat16),
        ],
        name="attend",
    )(where, *blocks)
    got = lax.all_to_all(parts.reshape(NY, rows, 3 * VD), "y", 0, 0, tiled=True)
    means = merged(got)
    diff = means[0] - second_weight[0] * means[1]
    scale_inv = lax.rsqrt(jnp.mean(diff * diff, axis=-1, keepdims=True) + eps)
    attended = (diff * scale_inv * head_gain * 0.8).astype(jnp.bfloat16)
    proj = summed_over_tp(
        jnp.dot(attended, out_weight, preferred_element_type=jnp.float32).astype(jnp.bfloat16)
    )
    mid = (residual.astype(jnp.float32) + proj.astype(jnp.float32)).astype(jnp.bfloat16)
    normed_all = lax.all_gather(normalize(mid, norm_gain), TP, axis=0, tiled=True)
    count = lax.axis_size("z") * lax.axis_size("y")
    rim_rows = lax.ppermute(normed_all[rows - 8 :], SP, [(i, i + 1) for i in range(count - 1)])
    d = normed_all.shape[1]
    in_vmem = [
        pltpu.with_memory_space_constraint(v, pltpu.VMEM) for v in (normed_all, rim_rows)
    ]
    ffn = pl.pallas_call(
        ffn_kernel,
        out_shape=pltpu.VMEM((rows, d), jnp.bfloat16),
        in_specs=[VMEM, VMEM, pl.BlockSpec(memory_space=pl.ANY), VMEM, VMEM],
        out_specs=VMEM,
        scratch_shapes=[
            pltpu.VMEM((rows + rim_rows.shape[0], d), jnp.bfloat16),
            pltpu.VMEM((rows + rim_rows.shape[0], 2 * ff), jnp.bfloat16),
            pltpu.VMEM((all_w.shape[0], deep, width + tail), jnp.bfloat16),
            pltpu.VMEM((all_w.shape[0], deep // 2, LANES), jnp.bfloat16),
            pltpu.SemaphoreType.DMA((width // LANES + 1,)),
        ],
        compiler_params=pltpu.CompilerParams(vmem_limit_bytes=40 * 2**20),
        name="ffn",
    )(*in_vmem, pltpu.with_memory_space_constraint(all_w, pltpu.HBM), conv_weight, conv_bias)
    ffn_out = summed_over_tp(ffn)
    return (mid.astype(jnp.float32) + ffn_out.astype(jnp.float32)).astype(jnp.bfloat16)


def solution(mesh):
    finer = Mesh(mesh.devices.reshape(NZ, NY, mesh.shape["tp"] // 2, 2), ("z", "y", "x", "c"))
    in_specs = (
        P(SP_TP, None),
        P(SP, TP),
        P(SP, TP),
        P(SP, TP),
        P(TP),
        P(TP),
        P(TP, None),
        P(),
        P(SP, TP),
        P(SP, TP),
        P(None, TP),
        P(TP),
        P(TP, SP),
    )
    out_specs = P(SP_TP, None)
    return jax.shard_map(local, mesh=finer, in_specs=in_specs, out_specs=out_specs, check_vma=False)
```
